256 devices in a mesh: rep: 2 (over z_hi), fs: 16 (over z_lo, y), tp: 8 (over x, core).
Axes of the slice: x: 4, y: 4, z: 8 (z_hi: 2, z_lo: 4; z = z_hi * 4 + z_lo), core: 2. Of those that a mesh axis runs over, the one named last changes fastest.
Arguments:
- tokens: bfloat16 [49152, 2048], P(('rep', 'fs', 'tp')), may hold values from -6 to 6
- mix_gain_in: float32 [2048], replicated, may hold values from 0.1 to 1.9
- pool_weight: bfloat16 [4, 512, 512], P(None, 'fs'), may hold values from -0.25 to 0.25
- mix_gain_out: float32 [2048], replicated, may hold values from 0.1 to 1.9
- ffn_gain_in: float32 [2048], replicated, may hold values from 0.1 to 1.9
- gate_weight: bfloat16 [2048, 5632], P('fs', 'tp'), may hold values from -0.125 to 0.125
- up_weight: bfloat16 [2048, 5632], P('fs', 'tp'), may hold values from -0.125 to 0.125
- gate_taps: float32 [3, 5632], replicated, may hold values from -3.5 to 3.5
- up_taps: float32 [3, 5632], replicated, may hold values from -3.5 to 3.5
- down_weight: bfloat16 [5632, 2048], P('tp', 'fs'), may hold values from -0.078125 to 0.078125
- ffn_gain_out: float32 [2048], replicated, may hold values from 0.1 to 1.9
Outputs:
- mixed_out: bfloat16 [49152, 2048], P(('rep', 'fs', 'tp'))
The draws below stay inside these ranges and needn't reach their ends.
All inputs are finite; a program needn't handle non-finite values.
Results may differ from the reference program's by a relative error of at most 0.014.
Values may be sent and summed in bfloat16 or wider, within the bound.
A program may use at most 128 MiB of HBM per device.

```python
import jax
import jax.numpy as jnp
from jax import lax

D = 2048
FF = 5632
GROUPS = 4
CONV_WIDTH = 3
GC = 512
SEQ_LEN = 1536
SEQS = 32
TOKENS = 49152
N_TP = 8


def level_of(rng, dims, cuts, smallest, largest):
    level = 1.0
    for position, blocks in cuts:
        heights = jax.random.uniform(jax.random.fold_in(jax.random.fold_in(rng, 6), position), (blocks,), jnp.float32, smallest / len(cuts), largest / len(cuts))
        level = level * jnp.repeat(jnp.exp(heights), dims[position] // blocks).reshape((-1,) + (1,) * (len(dims) - 1 - position))
    return level


def bell_draw(own_key, dims, deviation, limit, cuts=(), kind=jnp.bfloat16):
    values = jax.random.normal(own_key, dims, jnp.float32) * deviation
    if len(cuts) > 0:
        values = level_of(own_key, dims, cuts, -0.22, 0.18) * values
    return jnp.clip(values, min=-limit, max=limit).astype(kind)


def setup_inputs(seed: int = 0) -> dict:
    key_of = jax.random.split(jax.random.key(seed), 12)
    return {
        "tokens": bell_draw(key_of[0], (TOKENS, D), 1.0, 6.0, ((0, 256),)),
        "mix_gain_in": jnp.clip(1.0 + 0.18 * jax.random.normal(key_of[1], (D,), jnp.float32), 0.1, 1.9),
        "pool_weight": bell_draw(key_of[2], (GROUPS, GC, GC), GC ** -0.5, 0.25, ((1, 16),)),
        "mix_gain_out": jnp.clip(1.0 + 0.18 * jax.random.normal(key_of[3], (D,), jnp.float32), 0.1, 1.9),
        "ffn_gain_in": jnp.clip(1.0 + 0.18 * jax.random.normal(key_of[4], (D,), jnp.float32), 0.1, 1.9),
        "gate_weight": bell_draw(key_of[5], (D, FF), D ** -0.5, 0.125, ((0, 16), (1, 8))),
        "up_weight": bell_draw(key_of[6], (D, FF), D ** -0.5, 0.125, ((0, 16), (1, 8))),
        "gate_taps": bell_draw(key_of[7], (CONV_WIDTH, FF), CONV_WIDTH ** -0.5, 3.5, (), jnp.float32),
        "up_taps": bell_draw(key_of[8], (CONV_WIDTH, FF), CONV_WIDTH ** -0.5, 3.5, (), jnp.float32),
        "down_weight": bell_draw(key_of[9], (FF, D), FF ** -0.5, 0.078125, ((0, 8), (1, 16))),
        "ffn_gain_out": jnp.clip(1.0 + 0.18 * jax.random.normal(key_of[10], (D,), jnp.float32), 0.1, 1.9),
    }


pool_spans = (2, 4, 8, 16)
rms_eps = 1e-06

def rms_scale(values, gain):
    floats = values.astype(jnp.float32)
    return floats * lax.rsqrt(lax.optimization_barrier(jnp.mean(floats * floats, axis=-1, keepdims=True)) + rms_eps) * gain.astype(jnp.float32)

def pooled_gap(padded, first, count):
    margin = padded.shape[0] - count
    floats = padded.astype(jnp.float32)
    width = padded.shape[1] // len(pool_spans)
    where = first + jnp.arange(count, dtype=jnp.int32)
    pieces = []
    for group, span in enumerate(pool_spans):
        block = floats[:, group * width:(group + 1) * width]
        total = jnp.zeros((count, width), jnp.float32)
        for back in range(span):
            total = total + block[margin - back:margin - back + count]
        divisor = jnp.minimum(where + 1, span).astype(jnp.float32)
        pieces.append(total / divisor[:, None] - block[margin:])
    return jnp.concatenate(pieces, axis=1).astype(jnp.bfloat16)

def causal_taps(pre, taps):
    width = taps.shape[0]
    floats = pre.astype(jnp.float32)
    padded = jnp.concatenate([jnp.zeros((width - 1, pre.shape[1]), jnp.float32), floats], axis=0)
    total = jnp.zeros(floats.shape, jnp.float32)
    for offset in range(width):
        total = total + taps[offset].astype(jnp.float32) * padded[offset:offset + pre.shape[0]]
    return total

def reference(tokens, mix_gain_in, pool_weight, mix_gain_out, ffn_gain_in, gate_weight, up_weight, gate_taps, up_taps, down_weight, ffn_gain_out):
    margin = max(pool_spans) - 1

    def one_sequence(rows):
        normed = rms_scale(rows, mix_gain_in).astype(jnp.bfloat16)
        padded = jnp.concatenate([jnp.zeros((margin, D), jnp.bfloat16), normed], axis=0)
        gap = pooled_gap(padded, 0, SEQ_LEN)
        mixed = jnp.einsum('rgc,gcj->rgj', gap.reshape(SEQ_LEN, GROUPS, GC).astype(jnp.float32), pool_weight.astype(jnp.float32))
        mixed = mixed.reshape(SEQ_LEN, D).astype(jnp.bfloat16)
        after_mix = rows.astype(jnp.float32) + rms_scale(mixed, mix_gain_out)
        channel_in = rms_scale(after_mix, ffn_gain_in).astype(jnp.bfloat16)
        gate_pre = jnp.dot(channel_in, gate_weight, preferred_element_type=jnp.float32).astype(jnp.bfloat16)
        up_pre = jnp.dot(channel_in, up_weight, preferred_element_type=jnp.float32).astype(jnp.bfloat16)
        gate_conv = causal_taps(gate_pre, gate_taps)
        up_conv = causal_taps(up_pre, up_taps)
        hidden = (jax.nn.gelu(gate_conv, approximate=True) * up_conv).astype(jnp.bfloat16)
        partial_value = jnp.einsum('rtf,tfd->rtd', hidden.reshape(SEQ_LEN, N_TP, FF // N_TP).astype(jnp.float32), down_weight.reshape(N_TP, FF // N_TP, D).astype(jnp.float32)).astype(jnp.bfloat16)
        channel_out = lax.optimization_barrier(jnp.sum(partial_value.astype(jnp.float32), axis=1))
        return (after_mix + rms_scale(channel_out, ffn_gain_out)).astype(jnp.bfloat16)
    result = lax.map(one_sequence, tokens.reshape(SEQS, SEQ_LEN, D))
    return result.reshape(TOKENS, D)
```

```python
import functools

import jax
import jax.numpy as jnp
from jax import lax
from jax.experimental import pallas as pl
from jax.experimental.pallas import tpu as pltpu
from jax.sharding import PartitionSpec as P

MESH = pl.DeviceIdType.MESH
eps = 1e-06
ROWS = 192
HALO = 32
EXT = ROWS + HALO
OUTR = ROWS + 16
D = 2048
W = 704
WP = 768
GW = 2 * W
MAIN = 640
LANES = 128


def ring(value, n):
    return lax.rem(value + n, n)


class Gather:
    def __init__(self, piece, bundle, other, p, s, devs, partner, ssem, rsem):
        self.piece, self.bundle, self.other = piece, bundle, other
        self.p, self.s = p, s
        self.pu, self.pd, self.su, self.sd = devs
        self.partner = partner
        self.ssem, self.rsem = ssem, rsem
        self.sent = []

    def send(self, ref, dev, k):
        copy = pltpu.make_async_remote_copy(ref, ref, self.ssem.at[k], self.rsem.at[k], device_id=dev, device_id_type=MESH)
        copy.start()
        self.sent.append(copy)

    def recv(self, ref, k):
        pltpu.make_async_remote_copy(
            ref, ref, self.ssem.at[k], self.rsem.at[k], device_id=self.partner, device_id_type=MESH
        ).wait_recv()

    def s1(self):
        own = self.piece(self.p, None)
        self.send(own, self.pu, 0)
        self.send(own, self.pd, 1)

    def s2(self):
        low, high = ring(self.p - 1, 4), ring(self.p + 1, 4)
        self.recv(self.piece(low, None), 0)
        self.send(self.piece(low, 0), self.pu, 2)
        self.recv(self.piece(high, None), 1)
        self.send(self.piece(high, 1), self.pd, 3)

    def s3(self):
        far = ring(self.p + 2, 4)
        self.recv(self.piece(far, 0), 2)
        self.recv(self.piece(far, 1), 3)
        own = self.bundle(self.s, None)
        self.send(own, self.su, 4)
        self.send(own, self.sd, 5)
        self.send(own, self.partner, 8)

    def s4(self):
        low, high = ring(self.s - 1, 4), ring(self.s + 1, 4)
        self.recv(self.bundle(low, None), 4)
        self.send(self.bundle(low, 0), self.su, 6)
        self.recv(self.bundle(high, None), 5)
        self.send(self.bundle(high, 1), self.sd, 7)
        self.send(self.bundle(low, None), self.partner, 9)
        self.send(self.bundle(high, None), self.partner, 10)

    def s5(self):
        far = ring(self.s + 2, 4)
        self.recv(self.bundle(far, 0), 6)
        self.recv(self.bundle(far, 1), 7)
        self.send(self.bundle(far, None), self.partner, 11)

    def join(self):
        for k, off in ((8, 0), (9, -1), (10, 1), (11, 2)):
            self.recv(self.other(ring(self.s + off, 4)), k)

    def drain(self):
        for copy in self.sent:
            copy.wait_send()


def layer(
    tokens, pool_w, gu_w, dn_w, taps, gains, out,
    XB, NB, GAP, MIX, POOL, GU, DN, X, PRE, HID, SB, RB, R, AM,
    loc_sem, g_ssem, g_rsem, x_ssem, x_rsem, barrier_unused=None,
):
    rep, fs, tp = lax.axis_index("rep"), lax.axis_index("fs"), lax.axis_index("tp")
    zl, y = lax.div(fs, 4), lax.rem(fs, 4)
    z = rep * 4 + zl
    x, c = lax.div(tp, 2), lax.rem(tp, 2)

    def at_y(d):
        return (rep, zl * 4 + ring(y + d, 4), tp)

    def at_z(d):
        zn = ring(z + d, 8)
        return (lax.div(zn, 4), lax.rem(zn, 4) * 4 + y, tp)

    def at_tp(t):
        return (rep, fs, t)

    partner = at_tp(x * 2 + (1 - c))
    x_up, x_down = at_tp(ring(x + 1, 4) * 2 + c), at_tp(ring(x - 1, 4) * 2 + c)
    after = at_tp(ring(tp + 1, 8))
    cross = at_tp(ring(tp + 2 * c - 1, 8))
    y_up, y_down, z_up, z_down = at_y(1), at_y(-1), at_z(1), at_z(-1)

    mine = pl.ds(pl.multiple_of(c * GW, LANES), GW)
    theirs = pl.ds(pl.multiple_of((1 - c) * GW, LANES), GW)
    local = [
        pltpu.make_async_copy(tokens, XB.at[x, pl.ds(HALO, ROWS)], loc_sem.at[0]),
        pltpu.make_async_copy(pool_w.at[pl.ds(c * 2, 2)], POOL.at[pl.ds(c * 2, 2), zl, y], loc_sem.at[1]),
        pltpu.make_async_copy(gu_w, GU.at[zl, y, :, mine], loc_sem.at[2]),
        pltpu.make_async_copy(dn_w, DN.at[c, zl, y, pl.ds(0, W)], loc_sem.at[3]),
    ]
    for copy in local:
        copy.start()

    barrier = pltpu.get_barrier_semaphore()
    greeted = (partner, x_up, x_down, cross, y_up, y_down, z_up, z_down)
    for dev in greeted:
        pl.semaphore_signal(barrier, inc=1, device_id=dev, device_id_type=MESH)
    DN[:, :, :, W:WP, :] = jnp.zeros((2, 4, 4, WP - W, LANES), jnp.bfloat16)
    pl.semaphore_wait(barrier, len(greeted))
    for copy in local:
        copy.wait()

    def gathers(piece_a, bundle_a, other_a, piece_b, bundle_b, other_b, n):
        yz = (y_up, y_down, z_up, z_down)
        zy = (z_up, z_down, y_up, y_down)
        return (
            Gather(piece_a, bundle_a, other_a, y, zl, yz, partner, g_ssem.at[n], g_rsem.at[n]),
            Gather(piece_b, bundle_b, other_b, zl, y, zy, partner, g_ssem.at[n + 1], g_rsem.at[n + 1]),
        )

    def cut(start, size, sub):
        return pl.ds(start, size) if sub is None else pl.ds(start + sub * (size // 2), size // 2)

    pool = gathers(
        lambda p, sub: POOL.at[2 * c, zl, p, cut(0, 32, sub)],
        lambda s, sub: POOL.at[2 * c, s, :, cut(0, 32, sub)],
        lambda s: POOL.at[2 * (1 - c), s],
        lambda p, sub: POOL.at[2 * c + 1, p, y, cut(0, 32, sub)],
        lambda s, sub: POOL.at[2 * c + 1, :, s, cut(0, 32, sub)],
        lambda s: POOL.at[2 * (1 - c) + 1, :, s],
        0,
    )
    gu = gathers(
        lambda p, sub: GU.at[zl, p, cut(0, 64, sub), mine],
        lambda s, sub: GU.at[s, :, cut(0, 64, sub), mine],
        lambda s: GU.at[s, :, pl.ds(0, 64), theirs],
        lambda p, sub: GU.at[p, y, cut(64, 64, sub), mine],
        lambda s, sub: GU.at[:, s, cut(64, 64, sub), mine],
        lambda s: GU.at[:, s, pl.ds(64, 64), theirs],
        2,
    )
    dn = gathers(
        lambda p, sub: DN.at[c, zl, p, cut(0, 352, sub)],
        lambda s, sub: DN.at[c, s, :, cut(0, 352, sub)],
        lambda s: DN.at[1 - c, s, :, pl.ds(0, 352)],
        lambda p, sub: DN.at[c, p, y, cut(352, 352, sub)],
        lambda s, sub: DN.at[c, :, s, cut(352, 352, sub)],
        lambda s: DN.at[1 - c, :, s, pl.ds(352, 352)],
        4,
    )

    sent = []

    def push(src, dst, k, dev):
        copy = pltpu.make_async_remote_copy(src, dst, x_ssem.at[k], x_rsem.at[k], device_id=dev, device_id_type=MESH)
        copy.start()
        sent.append(copy)

    def arrived(dst, k):
        pltpu.make_async_remote_copy(
            dst, dst, x_ssem.at[k], x_rsem.at[k], device_id=partner, device_id_type=MESH
        ).wait_recv()

    low, high, far = ring(x - 1, 4), ring(x + 1, 4), ring(x + 2, 4)
    body = pl.ds(HALO, ROWS)
    head, tail = pl.ds(HALO, 96), pl.ds(HALO + 96, 96)
    last = pl.ds(EXT - HALO, HALO)
    top = pl.ds(0, HALO)

    push(XB.at[x, last], XB.at[ring(x + c, 4), top], 4, after)
    for g in pool:
        g.s1()
    push(XB.at[x, body], XB.at[x, body], 0, x_up)
    push(XB.at[x, body], XB.at[x, body], 1, x_down)
    for g in gu:
        g.s1()

    def side(m, slot):
        push(XB.at[ring(x + 1 - c + m, 4), last], XB.at[slot, top], 5 + m, partner)

    def mix(b, first_row, own):
        at_start = jnp.where(first_row == 0, 0.0, 1.0)
        XB[b, 0:HALO] = (XB[b, 0:HALO].astype(jnp.float32) * at_start).astype(jnp.bfloat16)

        def norm(i, _):
            r = pl.ds(pl.multiple_of(i * 16, 16), 16)
            v = XB[b, r, :].astype(jnp.float32)
            scale = lax.rsqrt(jnp.mean(v * v, axis=-1, keepdims=True) + eps)
            NB[r, :] = (v * scale * gains[0:1, :]).astype(jnp.bfloat16).astype(jnp.float32)
            return 0

        lax.fori_loop(0, EXT // 16, norm, 0)

        def pooled(i, _):
            r = pl.ds(pl.multiple_of(i * 16, 16), 16)
            both = pl.ds(pl.multiple_of(i * 16, 16), 32)
            where = first_row + i * 16 - 16 + lax.broadcasted_iota(jnp.int32, (16, LANES), 0)
            for g in range(4):
                span = 2 << g
                block = NB[both, g * 512:(g + 1) * 512]
                total = block
                for k in range(g + 1):
                    total = total + pltpu.roll(total, 1 << k, 0)
                inverse = 1.0 / jnp.clip(where + 1, 1, span).astype(jnp.float32)
                inverse = jnp.concatenate([inverse] * 4, axis=1)
                GAP[r, g * 512:(g + 1) * 512] = (total[16:] * inverse - block[16:]).astype(jnp.bfloat16)
            return 0

        lax.fori_loop(0, OUTR // 16, pooled, 0)
        for g in range(4):
            cols = slice(g * 512, (g + 1) * 512)
            MIX[:, cols] = jnp.dot(
                GAP[:, cols], POOL[g].reshape(512, 512), preferred_element_type=jnp.float32
            ).astype(jnp.bfloat16)

        def finish(i, _):
            r = pl.ds(pl.multiple_of(i * 16, 16), 16)
            v = MIX[r, :].astype(jnp.float32)
            scale = lax.rsqrt(jnp.mean(v * v, axis=-1, keepdims=True) + eps)
            t = XB[b, pl.ds(pl.multiple_of(i * 16 + 16, 16), 16), :].astype(jnp.float32)
            a = t + v * scale * gains[1:2, :]
            if own:
                AM[r, :] = a
            scale = lax.rsqrt(jnp.mean(a * a, axis=-1, keepdims=True) + eps)
            X[b, r, :] = (a * scale * gains[2:3, :]).astype(jnp.bfloat16)
            return 0

        lax.fori_loop(0, OUTR // 16, finish, 0)

    def start_of(b):
        return (2 * b + c) * ROWS

    for g in pool:
        g.s2()
    for g in pool:
        g.s3()
    for g in gu:
        g.s2()
    for g in pool:
        g.s4()
    for g in gu:
        g.s3()
    for g in pool:
        g.s5()
    for g in dn:
        g.s1()
    for g in pool:
        g.join()
    arrived(XB.at[x, top], 4)
    mix(x, start_of(x), True)
    for g in dn:
        g.s2()
    arrived(XB.at[low, body], 0)
    push(XB.at[low, head], XB.at[low, head], 2, x_up)
    arrived(XB.at[high, body], 1)
    push(XB.at[high, tail], XB.at[high, tail], 3, x_down)
    side(0, high)
    arrived(XB.at[high, top], 5)
    mix(high, start_of(high), False)
    for g in gu:
        g.s4()
    for g in dn:
        g.s3()
    arrived(XB.at[far, head], 2)
    arrived(XB.at[far, tail], 3)
    side(1, far)
    side(2, low)
    arrived(XB.at[far, top], 6)
    mix(far, start_of(far), False)
    arrived(XB.at[low, top], 7)
    mix(low, start_of(low), False)
    for g in gu:
        g.s5()
    for g in gu:
        g.join()

    def hidden_of(q, _):
        b = ring(x + 2 + q, 4)

        def project(j, _):
            cols = pl.ds(pl.multiple_of(j * 256, 256), 256)
            w = GU[:, :, :, cols].reshape(D, 256)
            PRE[:, cols] = jnp.dot(X[b], w, preferred_element_type=jnp.float32).astype(jnp.bfloat16).astype(jnp.float32)
            return 0

        lax.fori_loop(0, 2 * GW // 256, project, 0)

        def conv(first, taps_at, base, row):
            total = None
            for k in range(3):
                v = PRE[14 + row + k:14 + row + k + 48, pl.ds(first, LANES)]
                term = taps[base + k:base + k + 1, pl.ds(taps_at, LANES)] * v
                total = term if total is None else total + term
            return total

        def act(gate, up):
            inner = 0.7978845608028654 * (gate + 0.044715 * gate * gate * gate)
            return 0.5 * gate * (1.0 + jnp.tanh(inner)) * up

        for h in range(2):
            def main(t, _):
                to = pl.multiple_of(t * LANES, LANES)
                for row in range(0, ROWS, 48):
                    gate = conv(pl.multiple_of(h * GW + to, LANES), pl.multiple_of(h * WP + to, LANES), 0, row)
                    up = conv(pl.multiple_of(h * GW + MAIN + to, LANES), pl.multiple_of(h * WP + to, LANES), 3, row)
                    HID[b, h, row:row + 48, pl.ds(to, LANES)] = act(gate, up).astype(jnp.bfloat16)
                return 0

            lax.fori_loop(0, MAIN // LANES, main, 0)
            inside = lax.broadcasted_iota(jnp.int32, (48, LANES), 1) < 64
            for row in range(0, ROWS, 48):
                gate = conv(h * GW + 2 * MAIN, h * WP + MAIN, 0, row)
                up = pltpu.roll(conv(h * GW + 2 * MAIN, h * WP + MAIN, 3, row), 64, 1)
                HID[b, h, row:row + 48, MAIN:WP] = jnp.where(inside, act(gate, up), 0.0).astype(jnp.bfloat16)
        return 0

    lax.fori_loop(0, 1, hidden_of, 0)
    for g in dn:
        g.s4()
    lax.fori_loop(1, 4, hidden_of, 0)
    for g in dn:
        g.s5()
    for g in dn:
        g.join()

    def down(b):
        def part(j, _):
            total = None
            zz, yy = lax.div(j, 2), lax.rem(j, 2) * 2
            for h in range(2):
                w = jnp.concatenate([DN[h, zz, yy], DN[h, zz, yy + 1]], axis=1)
                term = jnp.dot(HID[b, h], w, preferred_element_type=jnp.float32)
                total = term if total is None else total + term
            SB[b, :, pl.ds(pl.multiple_of(j * 256, 256), 256)] = total.astype(jnp.bfloat16)
            return 0

        lax.fori_loop(0, 8, part, 0)

    def relay(b, start, k):
        def add(i, _):
            r = pl.ds(pl.multiple_of(start + i * 16, 16), 16)
            q = pl.ds(pl.multiple_of(i * 16, 16), 16)
            SB[b, r, :] = (SB[b, r, :].astype(jnp.float32) + RB[k, q, :].astype(jnp.float32)).astype(jnp.bfloat16)
            return 0

        lax.fori_loop(0, 6, add, 0)

    first, second = pl.ds(0, 96), pl.ds(96, 96)
    down(far)
    push(SB.at[far, first], RB.at[0], 8, x_up)
    push(SB.at[far, second], RB.at[1], 9, x_down)
    down(high)
    push(SB.at[high, second], R.at[0, second], 10, x_up)
    down(low)
    push(SB.at[low, first], R.at[1, first], 11, x_down)
    down(x)
    arrived(RB.at[0], 8)
    relay(high, 0, 0)
    push(SB.at[high, first], R.at[0, first], 12, x_up)
    arrived(RB.at[1], 9)
    relay(low, 96, 1)
    push(SB.at[low, second], R.at[1, second], 13, x_down)

    def last_rows(i, _):
        r = pl.ds(pl.multiple_of(i * 16, 16), 16)
        v = SB[x, r, :].astype(jnp.float32) + R[0, r, :].astype(jnp.float32) + R[1, r, :].astype(jnp.float32)
        scale = lax.rsqrt(jnp.mean(v * v, axis=-1, keepdims=True) + eps)
        a = AM[pl.ds(pl.multiple_of(i * 16 + 16, 16), 16), :]
        out[r, :] = (a + v * scale * gains[3:4, :]).astype(jnp.bfloat16)
        return 0

    arrived(R.at[0, second], 10)
    arrived(R.at[1, first], 11)
    arrived(R.at[0, first], 12)
    arrived(R.at[1, second], 13)
    lax.fori_loop(0, ROWS // 16, last_rows, 0)
    for copy in sent:
        copy.wait_send()
    for pair in (pool, gu, dn):
        for g in pair:
            g.drain()


def shards(
    tokens,
    mix_gain_in,
    pool_weight,
    mix_gain_out,
    ffn_gain_in,
    gate_weight,
    up_weight,
    gate_taps,
    up_taps,
    down_weight,
    ffn_gain_out,
):
    x = lax.axis_index("tp") // 2
    gu = jnp.concatenate(
        [gate_weight[:, :MAIN], up_weight[:, :MAIN], gate_weight[:, MAIN:], up_weight[:, MAIN:]], axis=1
    )
    gate_own = lax.dynamic_slice_in_dim(gate_taps, x * GW, GW, 1).reshape(3, 2, W)
    up_own = lax.dynamic_slice_in_dim(up_taps, x * GW, GW, 1).reshape(3, 2, W)
    blank = jnp.zeros((3, 2, WP - W), jnp.float32)
    gate_own = jnp.concatenate([gate_own, blank], axis=2)
    up_own = jnp.concatenate([up_own[:, :, :MAIN], blank, up_own[:, :, MAIN:]], axis=2)
    taps = jnp.pad(jnp.concatenate([gate_own, up_own], axis=0), ((0, 2), (0, 0), (0, 0))).reshape(8, 2 * WP)
    gains = jnp.stack([mix_gain_in, mix_gain_out, ffn_gain_in, ffn_gain_out])
    anywhere = pl.BlockSpec(memory_space=pl.ANY)
    vmem = pl.BlockSpec(memory_space=pltpu.VMEM)
    bf16, f32 = jnp.bfloat16, jnp.float32
    return pl.pallas_call(
        layer,
        out_shape=jax.ShapeDtypeStruct((ROWS, D), bf16),
        in_specs=[anywhere, anywhere, anywhere, anywhere, vmem, vmem],
        out_specs=vmem,
        scratch_shapes=[
            pltpu.VMEM((4, EXT, D), bf16),
            pltpu.VMEM((EXT, D), f32),
            pltpu.VMEM((OUTR, D), bf16),
            pltpu.VMEM((OUTR, D), bf16),
            pltpu.VMEM((4, 4, 4, 32, 512), bf16),
            pltpu.VMEM((4, 4, 128, 2 * GW), bf16),
            pltpu.VMEM((2, 4, 4, WP, LANES), bf16),
            pltpu.VMEM((4, OUTR, D), bf16),
            pltpu.VMEM((OUTR, 2 * GW), f32),
            pltpu.VMEM((4, 2, ROWS, WP), bf16),
            pltpu.VMEM((4, ROWS, D), bf16),
            pltpu.VMEM((2, 96, D), bf16),
            pltpu.VMEM((2, ROWS, D), bf16),
            pltpu.VMEM((OUTR, D), f32),
            pltpu.SemaphoreType.DMA((4,)),
            pltpu.SemaphoreType.DMA((6, 12)),
            pltpu.SemaphoreType.DMA((6, 12)),
            pltpu.SemaphoreType.DMA((14,)),
            pltpu.SemaphoreType.DMA((14,)),
        ],
        compiler_params=pltpu.CompilerParams(collective_id=0, has_side_effects=True, vmem_limit_bytes=60 * 1024 * 1024),
    )(tokens, pool_weight, gu, down_weight, taps, gains)


def solution(mesh):
    in_specs = (
        P(("rep", "fs", "tp"), None),
        P(),
        P(None, "fs", None),
        P(),
        P(),
        P("fs", "tp"),
        P("fs", "tp"),
        P(),
        P(),
        P("tp", "fs"),
        P(),
    )
    out_specs = P(("rep", "fs", "tp"), None)
    return jax.shard_map(shards, mesh=mesh, in_specs=in_specs, out_specs=out_specs, check_vma=False)
```

```python
import jax
import jax.numpy as jnp
from jax import lax
from jax.experimental import pallas as pl
from jax.experimental.pallas import tpu as pltpu
from jax.sharding import PartitionSpec as P

MESH = pl.DeviceIdType.MESH
eps = 1e-06
ROWS = 192
HALO = 32
EXT = ROWS + HALO
OUTR = ROWS + 16
D = 2048
W = 704
WP = 768
GW = 2 * W
MAIN = 640
LANES = 128


def ring(value, n):
    return lax.rem(value + n, n)


class Flow:
    def __init__(self, piece, bundle, block, other, p, s, devs, partner, ssem, rsem):
        self.piece, self.bundle, self.block, self.other = piece, bundle, block, other
        self.s = s
        self.columns = [ring(p + k, 4) for k in (0, -1, 1, 2)]
        self.pu, self.pd, self.su, self.sd, self.pfar, self.sfar = devs
        self.partner = partner
        self.ssem, self.rsem = ssem, rsem

    def send(self, ref, dev, k, n):
        pltpu.make_async_remote_copy(
            ref, ref, self.ssem.at[k], self.rsem.at[n], device_id=dev, device_id_type=MESH
        ).start()

    def seen(self, ref, k, n):
        return pltpu.make_async_remote_copy(
            ref, ref, self.ssem.at[k], self.rsem.at[n], device_id=self.partner, device_id_type=MESH
        )

    def recv(self, ref, n):
        self.seen(ref, 0, n).wait_recv()


class Direct(Flow):
    def spread(self, j):
        col = self.columns[j]
        ref = self.piece(col, self.s, None)
        self.send(ref, self.su, 1, 3)
        self.send(ref, self.sd, 1, 4)
        self.send(self.piece(col, self.s, 0), self.sfar[0], 1, 5)
        self.send(self.piece(col, self.s, 1), self.sfar[1], 1, 5)

    def start(self):
        col = self.columns[0]
        ref = self.piece(col, self.s, None)
        self.send(ref, self.pu, 0, 0)
        self.send(ref, self.pd, 0, 1)
        self.send(self.piece(col, self.s, 0), self.pfar[0], 0, 2)
        self.send(self.piece(col, self.s, 1), self.pfar[1], 0, 2)
        self.spread(0)

    def p(self):
        for j in (1, 2, 3):
            self.recv(self.piece(self.columns[j], self.s, None), j - 1)
            self.spread(j)
        self.send(self.bundle(self.s), self.partner, 2, 6)

    def r(self):
        for k, off in ((3, -1), (4, 1), (5, 2)):
            ref = self.bundle(ring(self.s + off, 4))
            self.recv(ref, k)
            self.send(ref, self.partner, 2, 6)

    def join(self):
        self.recv(self.other(None), 6)

    def drain(self):
        for k, (m, n) in enumerate(((1, 3), (3, 4), (4, 4))):
            self.seen(self.block(m, n), k, 0).wait_send()


class Relay(Flow):
    def __init__(self, *args, split):
        super().__init__(*args)
        self.split = split

    def start_p(self):
        own = self.piece(self.columns[0], self.s, None)
        self.send(own, self.pu, 0, 0)
        self.send(own, self.pd, 0, 1)

    def spread(self, j):
        ref = self.piece(self.columns[j], self.s, None)
        self.send(ref, self.su, 2, 3 + 2 * j)
        self.send(ref, self.sd, 2, 4 + 2 * j)

    def start_s(self):
        self.spread(0)

    def give(self, off, k):
        self.send(self.bundle(ring(self.s + off, 4)), self.partner, 4, 12 + k * self.split)

    def p1f(self):
        low, high = self.columns[1], self.columns[2]
        self.recv(self.piece(low, self.s, None), 0)
        self.send(self.piece(low, self.s, 0), self.pu, 1, 2)
        self.recv(self.piece(high, self.s, None), 1)
        self.send(self.piece(high, self.s, 1), self.pd, 1, 2)

    def p1s(self):
        self.spread(1)
        self.spread(2)

    def p2(self):
        self.recv(self.piece(self.columns[3], self.s, None), 2)
        self.spread(3)
        self.give(0, 0)

    def q(self, j):
        col = self.columns[j]
        low, high = ring(self.s - 1, 4), ring(self.s + 1, 4)
        self.recv(self.piece(col, low, None), 3 + 2 * j)
        self.send(self.piece(col, low, 0), self.su, 3, 11)
        self.recv(self.piece(col, high, None), 4 + 2 * j)
        self.send(self.piece(col, high, 1), self.sd, 3, 11)
        if j == 3:
            self.give(-1, 1)
            self.give(1, 2)

    def q0(self):
        self.q(0)

    def q1(self):
        self.q(1)

    def q2(self):
        self.q(2)

    def q3(self):
        self.q(3)

    def r(self):
        self.recv(self.bundle(ring(self.s + 2, 4)), 11)
        self.give(2, 3)

    def join(self):
        self.recv(self.other(None), 12)

    def join1(self):
        for k, off in ((0, 0), (1, -1), (2, 1)):
            self.recv(self.other(ring(self.s + off, 4)), 12 + k)

    def join2(self):
        self.recv(self.other(ring(self.s + 2, 4)), 15)

    def drain(self):
        for k, (m, n) in enumerate(((1, 2), (1, 1), (2, 4), (1, 4), (4, 4))):
            self.seen(self.block(m, n), k, 0).wait_send()


def layer(
    tokens, pool_w, gate_w, up_w, dn_w, gate_taps, up_taps, gain0, gain1, gain2, gain3, out,
    XB, SC, GAP, MIX, AF, POOL, GU, DN, X, P0, P1, HID, SB, RB, R, AM, TW, TG, TU, TAPS, GAINS,
    loc_sem, g_ssem, g_rsem, x_ssem, x_rsem,
):
    rep, fs, tp = lax.axis_index("rep"), lax.axis_index("fs"), lax.axis_index("tp")
    zl, y = lax.div(fs, 4), lax.rem(fs, 4)
    z = rep * 4 + zl
    x, c = lax.div(tp, 2), lax.rem(tp, 2)

    def at_y(d):
        return (rep, zl * 4 + ring(y + d, 4), tp)

    def at_z(d):
        zn = ring(z + d, 8)
        return (lax.div(zn, 4), lax.rem(zn, 4) * 4 + y, tp)

    def at_tp(t):
        return (rep, fs, t)

    partner = at_tp(x * 2 + (1 - c))
    x_up, x_down = at_tp(ring(x + 1, 4) * 2 + c), at_tp(ring(x - 1, 4) * 2 + c)
    after = at_tp(ring(tp + 1, 8))
    cross = at_tp(ring(tp + 2 * c - 1, 8))
    y_up, y_down, z_up, z_down = at_y(1), at_y(-1), at_z(1), at_z(-1)
    y_far, z_far = (at_y(2), at_y(2)), (at_z(2), at_z(-2))

    barrier = pltpu.get_barrier_semaphore()
    greeted = (partner, x_up, x_down, cross, y_up, y_down, z_up, z_down, y_far[0], *z_far)
    for dev in greeted:
        pl.semaphore_signal(barrier, inc=1, device_id=dev, device_id_type=MESH)

    def cut(start, size, sub):
        start, size = (start, size) if sub is None else (start + sub * (size // 2), size // 2)
        return pl.ds(start if isinstance(start, int) else pl.multiple_of(start, 16), size)

    mine = pl.ds(pl.multiple_of(c * GW, LANES), GW)
    theirs = pl.ds(pl.multiple_of((1 - c) * GW, LANES), GW)
    pairs = [
        (gate_w, TW.at[0]),
        (up_w, TW.at[1]),
        (tokens, XB.at[x, pl.ds(HALO, ROWS)]),
        (pool_w.at[pl.ds(c * 2, 2)], POOL.at[pl.ds(c * 2, 2), zl, y]),
        (dn_w.at[pl.ds(0, MAIN)], DN.at[zl, y, cut(c * WP, MAIN, None)]),
        (dn_w.at[pl.ds(MAIN, 64)], DN.at[zl, y, cut(MAIN + c * 64, 64, None)]),
        (gate_taps.at[:, pl.ds(pl.multiple_of(x * GW, LANES), GW)], TG),
        (up_taps.at[:, pl.ds(pl.multiple_of(x * GW, LANES), GW)], TU),
        (gain0, GAINS.at[0]),
        (gain1, GAINS.at[1]),
        (gain2, GAINS.at[2]),
        (gain3, GAINS.at[3]),
    ]
    local = [pltpu.make_async_copy(src, dst, loc_sem.at[k]) for k, (src, dst) in enumerate(pairs)]
    for copy in local:
        copy.start()
    for copy in local:
        copy.wait()
    turned = [TW[k].T for k in range(2)]
    for k in range(2):
        for t in range(5):
            at = pl.multiple_of(c * 1536 + t * 256 + k * LANES, LANES)
            GU[zl, y, :, pl.ds(at, LANES)] = turned[k][:, t * LANES:(t + 1) * LANES]
    ends = [w[:, MAIN:W] for w in turned]
    both = jnp.concatenate([ends[0], ends[1]], axis=1).astype(jnp.float32)
    swapped = jnp.concatenate([ends[1], ends[0]], axis=1).astype(jnp.float32)
    pick = jnp.where(c == 0, both, swapped)
    GU[zl, y, :, pl.ds(pl.multiple_of(1280 + c * LANES, LANES), LANES)] = pick.astype(jnp.bfloat16)
    for ref, base in ((TG, 0), (TU, 3)):
        v = ref[...]
        TAPS[base:base + 3, 0:MAIN] = v[:, 0:MAIN]
        TAPS[base:base + 3, MAIN:WP] = jnp.concatenate([v[:, MAIN:W], v[:, W + MAIN:GW]], axis=1)
        TAPS[base:base + 3, WP:GW] = v[:, W:W + MAIN]
    with jax.named_scope("barrier_wait"):
        pl.semaphore_wait(barrier, len(greeted))

    yz = (y_up, y_down, z_up, z_down, y_far, z_far)
    zy = (z_up, z_down, y_up, y_down, z_far, y_far)

    def region(ref, rows, cols=None):
        def at(i, j, sub=None):
            start, size = rows
            here = cut(start, size, sub)
            return ref.at[i, j, here] if cols is None else ref.at[i, j, here, cols]

        return at

    every = slice(None)

    def pair(make, mine_a, mine_b, theirs_a, theirs_b, n, **more):
        def block(at):
            return lambda m, k: at(pl.ds(0, m), pl.ds(0, k))

        return (
            make(
                lambda p, s, sub: mine_a(s, p, sub), lambda s: mine_a(s, every), block(mine_a),
                lambda s: theirs_a(every if s is None else s, every),
                y, zl, yz, partner, g_ssem.at[n], g_rsem.at[n], **more,
            ),
            make(
                lambda p, s, sub: mine_b(p, s, sub), lambda s: mine_b(every, s), block(mine_b),
                lambda s: theirs_b(every, every if s is None else s),
                zl, y, zy, partner, g_ssem.at[n + 1], g_rsem.at[n + 1], **more,
            ),
        )

    pool = pair(
        Direct,
        region(POOL.at[2 * c], (0, 32)), region(POOL.at[2 * c + 1], (0, 32)),
        region(POOL.at[2 * (1 - c)], (0, 32)), region(POOL.at[2 * (1 - c) + 1], (0, 32)),
        0,
    )
    gu = pair(
        Relay,
        region(GU, (0, 64), mine), region(GU, (64, 64), mine),
        region(GU, (0, 64), theirs), region(GU, (64, 64), theirs),
        2, split=0,
    )
    dn = pair(
        Relay,
        region(DN, (c * W, 352)), region(DN, (c * W + 352, 352)),
        region(DN, ((1 - c) * W, 352)), region(DN, ((1 - c) * W + 352, 352)),
        4, split=1,
    )

    def push(src, dst, k, dev):
        n = 0 if k < 4 else 1 if k < 8 else 2
        pltpu.make_async_remote_copy(
            src, dst, x_ssem.at[n], x_rsem.at[k], device_id=dev, device_id_type=MESH
        ).start()

    def pushed(ref, n):
        pltpu.make_async_remote_copy(
            ref, ref, x_ssem.at[n], x_rsem.at[0], device_id=partner, device_id_type=MESH
        ).wait_send()

    def arrived(dst, k):
        pltpu.make_async_remote_copy(
            dst, dst, x_ssem.at[0], x_rsem.at[k], device_id=partner, device_id_type=MESH
        ).wait_recv()

    low, high, far = ring(x - 1, 4), ring(x + 1, 4), ring(x + 2, 4)
    body = pl.ds(HALO, ROWS)
    head, tail = pl.ds(HALO, 96), pl.ds(HALO + 96, 96)
    last = pl.ds(EXT - HALO, HALO)
    top = pl.ds(0, HALO)

    def side(m, slot):
        push(XB.at[ring(x + 1 - c + m, 4), last], XB.at[slot, top], 5 + m, partner)

    def rows16(i):
        return pl.ds(pl.multiple_of(i * 16, 16), 16)

    def prep(b, first_row):
        at_start = jnp.where(first_row == 0, 0.0, 1.0)
        XB[b, 0:HALO] = (XB[b, 0:HALO].astype(jnp.float32) * at_start).astype(jnp.bfloat16)

        def scales(i, _):
            v = XB[b, rows16(i), :].astype(jnp.float32)
            scale = lax.rsqrt(jnp.mean(v * v, axis=-1, keepdims=True) + eps)
            SC[rows16(i), :] = jnp.broadcast_to(scale, (16, LANES))
            return 0

        lax.fori_loop(0, EXT // 16, scales, 0, unroll=7)
        where = first_row + lax.broadcasted_iota(jnp.int32, (16, LANES), 0)
        for g in range(4):
            span = 2 << g
            inverse = 1.0 / jnp.clip(where + 1, 1, span).astype(jnp.float32)

            def strip(t, _):
                cols = pl.ds(pl.multiple_of(g * 512 + t * LANES, LANES), LANES)
                v = XB[b, :, cols].astype(jnp.float32) * SC[...] * GAINS[0, :, cols]
                v = v.astype(jnp.bfloat16).astype(jnp.float32)
                total = v
                for k in range(g + 1):
                    total = total + pltpu.roll(total, 1 << k, 0)
                GAP[0:16, cols] = (total[16:32] * (1.0 / span) - v[16:32]).astype(jnp.bfloat16)
                GAP[16:32, cols] = (total[32:48] * inverse - v[32:48]).astype(jnp.bfloat16)
                GAP[32:OUTR, cols] = (total[48:] * (1.0 / span) - v[48:]).astype(jnp.bfloat16)
                return 0

            lax.fori_loop(0, 4, strip, 0)

    def post(b, keep):
        for g in range(4):
            cols = slice(g * 512, (g + 1) * 512)
            MIX[:, cols] = jnp.dot(
                GAP[:, cols], POOL[g].reshape(512, 512), preferred_element_type=jnp.float32
            ).astype(jnp.bfloat16)

        def scales(i, _):
            v = MIX[rows16(i), :].astype(jnp.float32)
            scale = lax.rsqrt(jnp.mean(v * v, axis=-1, keepdims=True) + eps)
            SC[rows16(i), :] = jnp.broadcast_to(scale, (16, LANES))
            return 0

        lax.fori_loop(0, OUTR // 16, scales, 0, unroll=13)

        def added(i, _):
            total = jnp.zeros((16, LANES), jnp.float32)
            scale = SC[rows16(i), :]
            for t in range(D // LANES):
                cols = slice(t * LANES, (t + 1) * LANES)
                v = MIX[rows16(i), cols].astype(jnp.float32)
                rows = pl.ds(pl.multiple_of(i * 16 + 16, 16), 16)
                a = XB[b, rows, cols].astype(jnp.float32) + v * scale * GAINS[1, :, cols]
                keep[rows16(i), cols] = a
                total = total + a * a
            scale = lax.rsqrt(jnp.sum(total, axis=-1, keepdims=True) * (1.0 / D) + eps)
            SC[rows16(i), :] = jnp.broadcast_to(scale, (16, LANES))
            return 0

        lax.fori_loop(0, OUTR // 16, added, 0)

        def scaled(i, _):
            scale = SC[rows16(i), :]
            for t in range(D // LANES):
                cols = slice(t * LANES, (t + 1) * LANES)
                X[b, rows16(i), cols] = (keep[rows16(i), cols] * scale * GAINS[2, :, cols]).astype(jnp.bfloat16)
            return 0

        lax.fori_loop(0, OUTR // 16, scaled, 0)

    def start_of(b):
        return (2 * b + c) * ROWS

    def hidden(b, begin, stop):
        def project(i, ref):
            w = GU[:, :, :, pl.ds(pl.multiple_of(i * 256, 256), 256)].reshape(D, 256)
            ref[...] = jnp.dot(X[b], w, preferred_element_type=jnp.float32).astype(jnp.bfloat16).astype(jnp.float32)

        def conv(v, taps_at, base):
            taps = TAPS[base:base + 3, pl.ds(taps_at, LANES)]
            return taps[0:1] * pltpu.roll(v, 2, 0) + taps[1:2] * pltpu.roll(v, 1, 0) + taps[2:3] * v

        def act(ref, i, ends):
            at = i * LANES if ends else pl.multiple_of(i * LANES, LANES)
            for row in (0, 96):
                gate, up = ref[row:row + 112, 0:LANES], ref[row:row + 112, LANES:]
                if ends:
                    lead = lax.broadcasted_iota(jnp.int32, (112, LANES), 1) < 64
                    gate, up = jnp.where(lead, gate, up), pltpu.roll(jnp.where(lead, up, gate), 64, 1)
                gate, up = conv(gate, at, 0)[16:], conv(up, at, 3)[16:]
                inner = 0.7978845608028654 * (gate + 0.044715 * gate * gate * gate)
                value = 0.5 * gate * (1.0 + jnp.tanh(inner)) * up
                HID[b, row:row + 96, pl.ds(at, LANES)] = value.astype(jnp.bfloat16)

        def order(i):
            return i + jnp.minimum(lax.div(i, 5), 1) - 6 * lax.div(i, 10)

        if begin == 0:
            project(0, P0)

        def two(i, _):
            project(order(2 * i + 1), P1)
            act(P0, order(2 * i), False)
            project(order(2 * i + 2), P0)
            act(P1, order(2 * i + 1), False)
            return 0

        lax.fori_loop(begin, stop, two, 0)
        if stop == 5:
            act(P0, 5, True)

    steps = [(0, 0), (0, 1), (0, -1), (1, 0), (-1, 0), (1, 1), (1, -1), (-1, 1)]
    steps += [(-1, -1), (2, 0), (2, 1), (2, -1), (0, 2), (1, 2), (-1, 2), (2, 2)]
    slots = [(ring(zl + dz, 4), ring(y + dy, 4)) for dz, dy in steps]

    def down(b, part):
        for k in range(8 * part, 8 * part + 8, 2):
            w = jnp.concatenate([DN[slots[k]], DN[slots[k + 1]]], axis=1)
            total = jnp.dot(HID[b], w, preferred_element_type=jnp.float32).astype(jnp.bfloat16)
            SB[b, k] = total[:, 0:LANES]
            SB[b, k + 1] = total[:, LANES:]

    def relay(b, start, k, part):
        rows = pl.ds(start, 96)

        def add(i, _):
            SB[b, i, rows] = (SB[b, i, rows].astype(jnp.float32) + RB[k, i].astype(jnp.float32)).astype(jnp.bfloat16)
            return 0

        lax.fori_loop(8 * part, 8 * part + 8, add, 0)

    first, second = pl.ds(0, 96), pl.ds(96, 96)
    push(XB.at[x, last], XB.at[ring(x + c, 4), top], 4, after)
    for g in pool:
        g.start()
    for g in gu:
        g.start_p()
    push(XB.at[x, body], XB.at[x, body], 0, x_up)
    push(XB.at[x, body], XB.at[x, body], 1, x_down)
    for g in pool:
        g.p()
    for g in gu:
        g.start_s()
    for g in gu:
        g.p1f()
    for g in gu:
        g.p1s()
    arrived(XB.at[x, top], 4)
    prep(x, start_of(x))
    for g in pool:
        g.r()
    for g in pool:
        g.join()
    post(x, AM)
    for g in gu:
        g.p2()
    for g in gu:
        g.q0()
    arrived(XB.at[low, body], 0)
    push(XB.at[low, head], XB.at[low, head], 2, x_up)
    arrived(XB.at[high, body], 1)
    push(XB.at[high, tail], XB.at[high, tail], 3, x_down)
    side(0, high)
    arrived(XB.at[high, top], 5)
    prep(high, start_of(high))
    post(high, AF)
    for g in gu:
        g.q1()
    for g in gu:
        g.q2()
    for g in dn:
        g.start_p()
    arrived(XB.at[far, head], 2)
    arrived(XB.at[far, tail], 3)
    side(1, far)
    side(2, low)
    arrived(XB.at[far, top], 6)
    for g in gu:
        g.q3()
    for g in dn:
        g.start_s()
    prep(far, start_of(far))
    post(far, AF)
    for g in dn:
        g.p1f()
    for g in dn:
        g.p1s()
    for g in gu:
        g.r()
    arrived(XB.at[low, top], 7)
    prep(low, start_of(low))
    for g in dn:
        g.p2()
    post(low, AF)
    for g in dn:
        g.q0()
    for g in gu:
        g.join()
    hidden(far, 0, 3)
    for g in dn:
        g.q1()
    for g in dn:
        g.q2()
    hidden(far, 3, 5)
    for g in dn:
        g.q3()
    hidden(high, 0, 3)
    for g in dn:
        g.join1()
    down(far, 0)
    push(SB.at[far, pl.ds(0, 8), first], RB.at[0, pl.ds(0, 8)], 8, x_up)
    push(SB.at[far, pl.ds(0, 8), second], RB.at[1, pl.ds(0, 8)], 9, x_down)
    for g in dn:
        g.r()
    hidden(high, 3, 5)
    for g in dn:
        g.join2()
    down(far, 1)
    push(SB.at[far, pl.ds(8, 8), first], RB.at[0, pl.ds(8, 8)], 14, x_up)
    push(SB.at[far, pl.ds(8, 8), second], RB.at[1, pl.ds(8, 8)], 15, x_down)
    down(high, 0)
    push(SB.at[high, pl.ds(0, 8), second], R.at[0, pl.ds(0, 8), second], 10, x_up)
    hidden(low, 0, 5)
    down(low, 0)
    push(SB.at[low, pl.ds(0, 8), first], R.at[1, pl.ds(0, 8), first], 11, x_down)
    down(high, 1)
    push(SB.at[high, pl.ds(8, 8), second], R.at[0, pl.ds(8, 8), second], 16, x_up)
    down(low, 1)
    push(SB.at[low, pl.ds(8, 8), first], R.at[1, pl.ds(8, 8), first], 17, x_down)
    arrived(RB.at[0, pl.ds(0, 8)], 8)
    relay(high, 0, 0, 0)
    push(SB.at[high, pl.ds(0, 8), first], R.at[0, pl.ds(0, 8), first], 12, x_up)
    arrived(RB.at[1, pl.ds(0, 8)], 9)
    relay(low, 96, 1, 0)
    push(SB.at[low, pl.ds(0, 8), second], R.at[1, pl.ds(0, 8), second], 13, x_down)
    arrived(RB.at[0, pl.ds(8, 8)], 14)
    relay(high, 0, 0, 1)
    push(SB.at[high, pl.ds(8, 8), first], R.at[0, pl.ds(8, 8), first], 18, x_up)
    arrived(RB.at[1, pl.ds(8, 8)], 15)
    relay(low, 96, 1, 1)
    push(SB.at[low, pl.ds(8, 8), second], R.at[1, pl.ds(8, 8), second], 19, x_down)
    hidden(x, 0, 5)
    down(x, 0)
    down(x, 1)

    def last_rows(i, _):
        r = rows16(i)
        total = jnp.zeros((16, LANES), jnp.float32)
        values = []
        for k in range(16):
            v = SB[x, k, r].astype(jnp.float32) + R[0, k, r].astype(jnp.float32) + R[1, k, r].astype(jnp.float32)
            values.append(v)
            total = total + v * v
        scale = lax.rsqrt(jnp.sum(total, axis=-1, keepdims=True) * (1.0 / D) + eps)
        for k in range(16):
            cols = pl.ds(pl.multiple_of((slots[k][0] * 4 + slots[k][1]) * LANES, LANES), LANES)
            a = AM[pl.ds(pl.multiple_of(i * 16 + 16, 16), 16), cols]
            out[r, cols] = (a + values[k] * scale * GAINS[3, :, cols]).astype(jnp.bfloat16)
        return 0

    arrived(R.at[0, pl.ds(0, 8), second], 10)
    arrived(R.at[1, pl.ds(0, 8), first], 11)
    arrived(R.at[0, pl.ds(0, 8), first], 12)
    arrived(R.at[1, pl.ds(0, 8), second], 13)
    arrived(R.at[0, pl.ds(8, 8), second], 16)
    arrived(R.at[1, pl.ds(8, 8), first], 17)
    arrived(R.at[0, pl.ds(8, 8), first], 18)
    arrived(R.at[1, pl.ds(8, 8), second], 19)
    lax.fori_loop(0, ROWS // 16, last_rows, 0, unroll=2)
    with jax.named_scope("drain"):
        pushed(XB.at[pl.ds(0, 3), pl.ds(0, ROWS)], 0)
        pushed(XB.at[0, pl.ds(0, 4 * HALO)], 1)
        pushed(SB.at[pl.ds(0, 3)], 2)
        for both in (pool, gu, dn):
            for g in both:
                g.drain()


def shards(
    tokens,
    mix_gain_in,
    pool_weight,
    mix_gain_out,
    ffn_gain_in,
    gate_weight,
    up_weight,
    gate_taps,
    up_taps,
    down_weight,
    ffn_gain_out,
):
    anywhere = pl.BlockSpec(memory_space=pl.ANY)
    vmem = pl.BlockSpec(memory_space=pltpu.VMEM)
    bf16, f32 = jnp.bfloat16, jnp.float32
    gains = [g.reshape(1, D) for g in (mix_gain_in, mix_gain_out, ffn_gain_in, ffn_gain_out)]
    return pl.pallas_call(
        layer,
        out_shape=jax.ShapeDtypeStruct((ROWS, D), bf16),
        in_specs=[anywhere] * 11,
        out_specs=vmem,
        scratch_shapes=[
            pltpu.VMEM((4, EXT, D), bf16),
            pltpu.VMEM((EXT, LANES), f32),
            pltpu.VMEM((OUTR, D), bf16),
            pltpu.VMEM((OUTR, D), bf16),
            pltpu.VMEM((OUTR, D), f32),
            pltpu.VMEM((4, 4, 4, 32, 512), bf16),
            pltpu.VMEM((4, 4, 128, 2 * GW), bf16),
            pltpu.VMEM((4, 4, GW, LANES), bf16),
            pltpu.VMEM((4, OUTR, D), bf16),
            pltpu.VMEM((OUTR, 256), f32),
            pltpu.VMEM((OUTR, 256), f32),
            pltpu.VMEM((4, ROWS, GW), bf16),
            pltpu.VMEM((4, 16, ROWS, LANES), bf16),
            pltpu.VMEM((2, 16, 96, LANES), bf16),
            pltpu.VMEM((2, 16, ROWS, LANES), bf16),
            pltpu.VMEM((OUTR, D), f32),
            pltpu.VMEM((2, W, LANES), bf16),
            pltpu.VMEM((3, GW), f32),
            pltpu.VMEM((3, GW), f32),
            pltpu.VMEM((8, GW), f32),
            pltpu.VMEM((4, 1, D), f32),
            pltpu.SemaphoreType.DMA((12,)),
            pltpu.SemaphoreType.DMA((6, 5)),
            pltpu.SemaphoreType.DMA((6, 16)),
            pltpu.SemaphoreType.DMA((3,)),
            pltpu.SemaphoreType.DMA((20,)),
        ],
        compiler_params=pltpu.CompilerParams(collective_id=0, has_side_effects=True, vmem_limit_bytes=60 * 1024 * 1024),
    )(tokens, pool_weight, gate_weight.T, up_weight.T, down_weight, gate_taps, up_taps, *gains)


def solution(mesh):
    in_specs = (
        P(("rep", "fs", "tp"), None),
        P(),
        P(None, "fs", None),
        P(),
        P(),
        P("fs", "tp"),
        P("fs", "tp"),
        P(),
        P(),
        P("tp", "fs"),
        P(),
    )
    out_specs = P(("rep", "fs", "tp"), None)
    return jax.shard_map(shards, mesh=mesh, in_specs=in_specs, out_specs=out_specs, check_vma=False)
```

```python
import jax
import jax.numpy as jnp
from jax import lax
from jax.experimental import pallas as pl
from jax.experimental.pallas import tpu as pltpu
from jax.sharding import PartitionSpec as P

MESH = pl.DeviceIdType.MESH
eps = 1e-06
ROWS = 192
HALO = 32
EXT = ROWS + HALO
OUTR = ROWS + 16
D = 2048
W = 704
WP = 768
GW = 2 * W
MAIN = 640
LANES = 128


def ring(value, n):
    return lax.rem(value + n, n)


class Flow:
    def __init__(self, piece, bundle, block, other, p, s, devs, partner, ssem, rsem):
        self.piece, self.bundle, self.block, self.other = piece, bundle, block, other
        self.s = s
        self.columns = [ring(p + k, 4) for k in (0, -1, 1, 2)]
        self.pu, self.pd, self.su, self.sd = devs
        self.partner = partner
        self.ssem, self.rsem = ssem, rsem

    def send(self, ref, dev, k, n):
        pltpu.make_async_remote_copy(
            ref, ref, self.ssem.at[k], self.rsem.at[n], device_id=dev, device_id_type=MESH
        ).start()

    def seen(self, ref, k, n):
        return pltpu.make_async_remote_copy(
            ref, ref, self.ssem.at[k], self.rsem.at[n], device_id=self.partner, device_id_type=MESH
        )

    def recv(self, ref, n):
        self.seen(ref, 0, n).wait_recv()


class Relay(Flow):
    def __init__(self, *args, split):
        super().__init__(*args)
        self.split = split

    def start_p(self):
        own = self.piece(self.columns[0], self.s, None)
        self.send(own, self.pu, 0, 0)
        self.send(own, self.pd, 0, 1)

    def spread(self, j):
        ref = self.piece(self.columns[j], self.s, None)
        self.send(ref, self.su, 2, 3 + 2 * j)
        self.send(ref, self.sd, 2, 4 + 2 * j)

    def start_s(self):
        self.spread(0)

    def give(self, off, k):
        self.send(self.bundle(ring(self.s + off, 4)), self.partner, 4, 12 + k * self.split)

    def p1f(self):
        low, high = self.columns[1], self.columns[2]
        self.recv(self.piece(low, self.s, None), 0)
        self.send(self.piece(low, self.s, 0), self.pu, 1, 2)
        self.recv(self.piece(high, self.s, None), 1)
        self.send(self.piece(high, self.s, 1), self.pd, 1, 2)

    def p1s(self):
        self.spread(1)
        self.spread(2)

    def p2(self):
        self.recv(self.piece(self.columns[3], self.s, None), 2)
        self.spread(3)
        self.give(0, 0)

    def q(self, j):
        col = self.columns[j]
        low, high = ring(self.s - 1, 4), ring(self.s + 1, 4)
        self.recv(self.piece(col, low, None), 3 + 2 * j)
        self.send(self.piece(col, low, 0), self.su, 3, self.landed(j))
        self.recv(self.piece(col, high, None), 4 + 2 * j)
        self.send(self.piece(col, high, 1), self.sd, 3, self.landed(j))
        if j == 3:
            self.give(-1, 1)
            self.give(1, 2)

    def q0(self):
        self.q(0)

    def q1(self):
        self.q(1)

    def q2(self):
        self.q(2)

    def q3(self):
        self.q(3)

    def landed(self, j):
        return 11 if j == 0 else 15 + j

    def far(self, j):
        ref = self.piece(self.columns[j], ring(self.s + 2, 4), None)
        self.recv(ref, self.landed(j))
        self.send(ref, self.partner, 4, 12 + 3 * self.split)

    def r012(self):
        for j in range(3):
            self.far(j)

    def r3(self):
        self.far(3)

    def join(self):
        self.recv(self.other(None), 12)

    def join1(self):
        for k, off in ((0, 0), (1, -1), (2, 1)):
            self.recv(self.other(ring(self.s + off, 4)), 12 + k)

    def join2(self):
        self.recv(self.other(ring(self.s + 2, 4)), 15)

    def drain(self):
        for k, (m, n) in enumerate(((1, 2), (1, 1), (2, 4), (1, 4), (4, 4))):
            self.seen(self.block(m, n), k, 0).wait_send()


def layer(
    tokens, pool_w, gate_w, up_w, dn_w, gate_taps, up_taps, gain0, gain1, gain2, gain3, out,
    XB, SC, GAP, MIX, AF, POOL, GU, DN, X, P0, P1, HID, SB, RB, R, AM, TW, TG, TU, TAPS, GAINS,
    loc_sem, g_ssem, g_rsem, x_ssem, x_rsem,
):
    rep, fs, tp = lax.axis_index("rep"), lax.axis_index("fs"), lax.axis_index("tp")
    zl, y = lax.div(fs, 4), lax.rem(fs, 4)
    z = rep * 4 + zl
    x, c = lax.div(tp, 2), lax.rem(tp, 2)

    def at_y(d):
        return (rep, zl * 4 + ring(y + d, 4), tp)

    def at_z(d):
        zn = ring(z + d, 8)
        return (lax.div(zn, 4), lax.rem(zn, 4) * 4 + y, tp)

    def at_tp(t):
        return (rep, fs, t)

    partner = at_tp(x * 2 + (1 - c))
    x_up, x_down = at_tp(ring(x + 1, 4) * 2 + c), at_tp(ring(x - 1, 4) * 2 + c)
    after = at_tp(ring(tp + 1, 8))
    cross = at_tp(ring(tp + 2 * c - 1, 8))
    y_up, y_down, z_up, z_down = at_y(1), at_y(-1), at_z(1), at_z(-1)

    barrier = pltpu.get_barrier_semaphore()
    greeted = (partner, x_up, x_down, cross, y_up, y_down, z_up, z_down)
    for dev in greeted:
        pl.semaphore_signal(barrier, inc=1, device_id=dev, device_id_type=MESH)

    def cut(start, size, sub):
        start, size = (start, size) if sub is None else (start + sub * (size // 2), size // 2)
        return pl.ds(start if isinstance(start, int) else pl.multiple_of(start, 16), size)

    mine = pl.ds(pl.multiple_of(c * GW, LANES), GW)
    theirs = pl.ds(pl.multiple_of((1 - c) * GW, LANES), GW)
    pairs = [
        (gate_w, TW.at[0]),
        (up_w, TW.at[1]),
        (tokens, XB.at[x, pl.ds(HALO, ROWS)]),
        (pool_w.at[pl.ds(c * 2, 2)], POOL.at[pl.ds(c * 2, 2), zl, y]),
        (dn_w.at[pl.ds(0, MAIN)], DN.at[zl, y, cut(c * WP, MAIN, None)]),
        (dn_w.at[pl.ds(MAIN, 64)], DN.at[zl, y, cut(MAIN + c * 64, 64, None)]),
        (gate_taps.at[:, pl.ds(pl.multiple_of(x * GW, LANES), GW)], TG),
        (up_taps.at[:, pl.ds(pl.multiple_of(x * GW, LANES), GW)], TU),
        (gain0, GAINS.at[0]),
        (gain1, GAINS.at[1]),
        (gain2, GAINS.at[2]),
        (gain3, GAINS.at[3]),
    ]
    local = [pltpu.make_async_copy(src, dst, loc_sem.at[k]) for k, (src, dst) in enumerate(pairs)]
    for copy in local:
        copy.start()
    for k in (2, 3):
        local[k].wait()

    def build():
        for k in (0, 1, 4, 5, 6, 7, 8, 9, 10, 11):
            local[k].wait()
        turned = [TW[k].T for k in range(2)]
        for k in range(2):
            for t in range(5):
                at = pl.multiple_of(c * 1536 + t * 256 + k * LANES, LANES)
                GU[zl, y, :, pl.ds(at, LANES)] = turned[k][:, t * LANES:(t + 1) * LANES]
        ends = [w[:, MAIN:W] for w in turned]
        both = jnp.concatenate([ends[0], ends[1]], axis=1).astype(jnp.float32)
        swapped = jnp.concatenate([ends[1], ends[0]], axis=1).astype(jnp.float32)
        pick = jnp.where(c == 0, both, swapped)
        GU[zl, y, :, pl.ds(pl.multiple_of(1280 + c * LANES, LANES), LANES)] = pick.astype(jnp.bfloat16)
        for ref, base in ((TG, 0), (TU, 3)):
            v = ref[...]
            TAPS[base:base + 3, 0:MAIN] = v[:, 0:MAIN]
            TAPS[base:base + 3, MAIN:WP] = jnp.concatenate([v[:, MAIN:W], v[:, W + MAIN:GW]], axis=1)
            TAPS[base:base + 3, WP:GW] = v[:, W:W + MAIN]

    with jax.named_scope("barrier_wait"):
        pl.semaphore_wait(barrier, len(greeted))

    yz = (y_up, y_down, z_up, z_down)
    zy = (z_up, z_down, y_up, y_down)

    def region(ref, rows, cols=None):
        def at(i, j, sub=None):
            start, size = rows
            here = cut(start, size, sub)
            return ref.at[i, j, here] if cols is None else ref.at[i, j, here, cols]

        return at

    every = slice(None)

    def pair(make, mine_a, mine_b, theirs_a, theirs_b, n, **more):
        def block(at):
            return lambda m, k: at(pl.ds(0, m), pl.ds(0, k))

        return (
            make(
                lambda p, s, sub: mine_a(s, p, sub), lambda s: mine_a(s, every), block(mine_a),
                lambda s: theirs_a(every if s is None else s, every),
                y, zl, yz, partner, g_ssem.at[n], g_rsem.at[n], **more,
            ),
            make(
                lambda p, s, sub: mine_b(p, s, sub), lambda s: mine_b(every, s), block(mine_b),
                lambda s: theirs_b(every, every if s is None else s),
                zl, y, zy, partner, g_ssem.at[n + 1], g_rsem.at[n + 1], **more,
            ),
        )

    pool = pair(
        Relay,
        region(POOL.at[2 * c], (0, 32)), region(POOL.at[2 * c + 1], (0, 32)),
        region(POOL.at[2 * (1 - c)], (0, 32)), region(POOL.at[2 * (1 - c) + 1], (0, 32)),
        0, split=0,
    )
    gu = pair(
        Relay,
        region(GU, (0, 64), mine), region(GU, (64, 64), mine),
        region(GU, (0, 64), theirs), region(GU, (64, 64), theirs),
        2, split=0,
    )
    dn = pair(
        Relay,
        region(DN, (c * W, 352)), region(DN, (c * W + 352, 352)),
        region(DN, ((1 - c) * W, 352)), region(DN, ((1 - c) * W + 352, 352)),
        4, split=1,
    )

    def push(src, dst, k, dev):
        n = 0 if k < 4 else 1 if k < 8 else 2
        pltpu.make_async_remote_copy(
            src, dst, x_ssem.at[n], x_rsem.at[k], device_id=dev, device_id_type=MESH
        ).start()

    def pushed(ref, n):
        pltpu.make_async_remote_copy(
            ref, ref, x_ssem.at[n], x_rsem.at[0], device_id=partner, device_id_type=MESH
        ).wait_send()

    def arrived(dst, k):
        pltpu.make_async_remote_copy(
            dst, dst, x_ssem.at[0], x_rsem.at[k], device_id=partner, device_id_type=MESH
        ).wait_recv()

    low, high, far = ring(x - 1, 4), ring(x + 1, 4), ring(x + 2, 4)
    body = pl.ds(HALO, ROWS)
    head, tail = pl.ds(HALO, 96), pl.ds(HALO + 96, 96)
    last = pl.ds(EXT - HALO, HALO)
    top = pl.ds(0, HALO)

    def side(m, slot):
        push(XB.at[ring(x + 1 - c + m, 4), last], XB.at[slot, top], 5 + m, partner)

    def rows16(i):
        return pl.ds(pl.multiple_of(i * 16, 16), 16)

    def prep(b, first_row):
        at_start = jnp.where(first_row == 0, 0.0, 1.0)
        XB[b, 0:HALO] = (XB[b, 0:HALO].astype(jnp.float32) * at_start).astype(jnp.bfloat16)

        def scales(i, _):
            v = XB[b, rows16(i), :].astype(jnp.float32)
            scale = lax.rsqrt(jnp.mean(v * v, axis=-1, keepdims=True) + eps)
            SC[rows16(i), :] = jnp.broadcast_to(scale, (16, LANES))
            return 0

        lax.fori_loop(0, EXT // 16, scales, 0, unroll=7)
        where = first_row + lax.broadcasted_iota(jnp.int32, (16, LANES), 0)
        for g in range(4):
            span = 2 << g
            inverse = 1.0 / jnp.clip(where + 1, 1, span).astype(jnp.float32)

            def strip(t, _):
                cols = pl.ds(pl.multiple_of(g * 512 + t * LANES, LANES), LANES)
                v = XB[b, :, cols].astype(jnp.float32) * SC[...] * GAINS[0, :, cols]
                v = v.astype(jnp.bfloat16).astype(jnp.float32)
                total = v
                for k in range(g + 1):
                    total = total + pltpu.roll(total, 1 << k, 0)
                GAP[0:16, cols] = (total[16:32] * (1.0 / span) - v[16:32]).astype(jnp.bfloat16)
                GAP[16:32, cols] = (total[32:48] * inverse - v[32:48]).astype(jnp.bfloat16)
                GAP[32:OUTR, cols] = (total[48:] * (1.0 / span) - v[48:]).astype(jnp.bfloat16)
                return 0

            lax.fori_loop(0, 4, strip, 0)

    def post(b, n, keep):
        for g in range(4):
            cols = slice(g * 512, (g + 1) * 512)
            MIX[:, cols] = jnp.dot(
                GAP[:, cols], POOL[g].reshape(512, 512), preferred_element_type=jnp.float32
            ).astype(jnp.bfloat16)

        def scales(i, _):
            v = MIX[rows16(i), :].astype(jnp.float32)
            scale = lax.rsqrt(jnp.mean(v * v, axis=-1, keepdims=True) + eps)
            SC[rows16(i), :] = jnp.broadcast_to(scale, (16, LANES))
            return 0

        lax.fori_loop(0, OUTR // 16, scales, 0, unroll=13)

        def added(i, _):
            total = jnp.zeros((16, LANES), jnp.float32)
            scale = SC[rows16(i), :]
            for t in range(D // LANES):
                cols = slice(t * LANES, (t + 1) * LANES)
                v = MIX[rows16(i), cols].astype(jnp.float32)
                rows = pl.ds(pl.multiple_of(i * 16 + 16, 16), 16)
                a = XB[b, rows, cols].astype(jnp.float32) + v * scale * GAINS[1, :, cols]
                keep[rows16(i), cols] = a
                total = total + a * a
            scale = lax.rsqrt(jnp.sum(total, axis=-1, keepdims=True) * (1.0 / D) + eps)
            SC[rows16(i), :] = jnp.broadcast_to(scale, (16, LANES))
            return 0

        lax.fori_loop(0, OUTR // 16, added, 0)

        def scaled(i, _):
            scale = SC[rows16(i), :]
            for t in range(D // LANES):
                cols = slice(t * LANES, (t + 1) * LANES)
                X[n, rows16(i), cols] = (keep[rows16(i), cols] * scale * GAINS[2, :, cols]).astype(jnp.bfloat16)
            return 0

        lax.fori_loop(0, OUTR // 16, scaled, 0)

    def start_of(b):
        return (2 * b + c) * ROWS

    def hidden(n, count, begin, stop):
        size = count * OUTR
        left = X[n] if count == 1 else X[n:n + count].reshape(size, D)

        def project(i, ref):
            w = GU[:, :, :, pl.ds(pl.multiple_of(i * 256, 256), 256)].reshape(D, 256)
            pre = jnp.dot(left, w, preferred_element_type=jnp.float32).astype(jnp.bfloat16).astype(jnp.float32)
            ref[0:size, :] = pre

        def conv(v, taps_at, base):
            taps = TAPS[base:base + 3, pl.ds(taps_at, LANES)]
            return taps[0:1] * pltpu.roll(v, 2, 0) + taps[1:2] * pltpu.roll(v, 1, 0) + taps[2:3] * v

        def act(ref, i, ends):
            at = i * LANES if ends else pl.multiple_of(i * LANES, LANES)
            for k in range(count):
                for row in (0, 96):
                    here = slice(k * OUTR + row, k * OUTR + row + 112)
                    gate, up = ref[here, 0:LANES], ref[here, LANES:]
                    if ends:
                        lead = lax.broadcasted_iota(jnp.int32, (112, LANES), 1) < 64
                        gate, up = jnp.where(lead, gate, up), pltpu.roll(jnp.where(lead, up, gate), 64, 1)
                    gate, up = conv(gate, at, 0)[16:], conv(up, at, 3)[16:]
                    inner = 0.7978845608028654 * (gate + 0.044715 * gate * gate * gate)
                    value = 0.5 * gate * (1.0 + jnp.tanh(inner)) * up
                    HID[n + k, row:row + 96, pl.ds(at, LANES)] = value.astype(jnp.bfloat16)

        def order(i):
            return i + jnp.minimum(lax.div(i, 5), 1) - 6 * lax.div(i, 10)

        if begin == 0:
            project(0, P0)

        def two(i, _):
            project(order(2 * i + 1), P1)
            act(P0, order(2 * i), False)
            project(order(2 * i + 2), P0)
            act(P1, order(2 * i + 1), False)
            return 0

        lax.fori_loop(begin, stop, two, 0)
        if stop == 5:
            act(P0, 5, True)

    steps = [(0, 0), (0, 1), (0, -1), (1, 0), (-1, 0), (1, 1), (1, -1), (-1, 1)]
    steps += [(-1, -1), (2, 0), (2, 1), (2, -1), (0, 2), (1, 2), (-1, 2), (2, 2)]
    slots = [(ring(zl + dz, 4), ring(y + dy, 4)) for dz, dy in steps]

    def down(b, part):
        for k in range(8 * part, 8 * part + 8, 2):
            w = jnp.concatenate([DN[slots[k]], DN[slots[k + 1]]], axis=1)
            total = jnp.dot(HID[b], w, preferred_element_type=jnp.float32).astype(jnp.bfloat16)
            SB[b, k] = total[:, 0:LANES]
            SB[b, k + 1] = total[:, LANES:]

    def relay(b, start, k, part):
        rows = pl.ds(start, 96)

        def add(i, _):
            SB[b, i, rows] = (SB[b, i, rows].astype(jnp.float32) + RB[k, i].astype(jnp.float32)).astype(jnp.bfloat16)
            return 0

        lax.fori_loop(8 * part, 8 * part + 8, add, 0)

    first, second = pl.ds(0, 96), pl.ds(96, 96)
    push(XB.at[x, last], XB.at[ring(x + c, 4), top], 4, after)
    for g in pool:
        g.start_p()
    for g in pool:
        g.start_s()
    push(XB.at[x, body], XB.at[x, body], 0, x_up)
    push(XB.at[x, body], XB.at[x, body], 1, x_down)
    build()
    for g in gu:
        g.start_p()
    for g in pool:
        g.p1f()
    for g in pool:
        g.p1s()
    arrived(XB.at[x, top], 4)
    prep(x, start_of(x))
    for g in pool:
        g.p2()
    for g in pool:
        g.q0()
    for g in pool:
        g.q1()
    for g in pool:
        g.q2()
    for g in gu:
        g.start_s()
    for g in gu:
        g.p1f()
    for g in pool:
        g.q3()
    for g in gu:
        g.p1s()
    for g in pool:
        g.r012()
    for g in pool:
        g.r3()
    arrived(XB.at[low, body], 0)
    push(XB.at[low, head], XB.at[low, head], 2, x_up)
    arrived(XB.at[high, body], 1)
    push(XB.at[high, tail], XB.at[high, tail], 3, x_down)
    side(0, high)
    for g in pool:
        g.join()
    post(x, 3, AM)
    for g in gu:
        g.p2()
    for g in gu:
        g.q0()
    arrived(XB.at[high, top], 5)
    prep(high, start_of(high))
    post(high, 1, AF)
    for g in gu:
        g.q1()
    for g in dn:
        g.start_p()
    for g in gu:
        g.q2()
    arrived(XB.at[far, head], 2)
    arrived(XB.at[far, tail], 3)
    side(1, far)
    side(2, low)
    arrived(XB.at[far, top], 6)
    for g in gu:
        g.q3()
    for g in dn:
        g.start_s()
    prep(far, start_of(far))
    post(far, 0, AF)
    arrived(XB.at[low, top], 7)
    prep(low, start_of(low))
    for g in dn:
        g.p1f()
    for g in dn:
        g.p1s()
    post(low, 2, AF)
    for g in gu:
        g.r012()
    for g in gu:
        g.r3()
    for g in gu:
        g.join()
    hidden(0, 1, 0, 1)
    for g in dn:
        g.p2()
    hidden(0, 1, 1, 3)
    for g in dn:
        g.q0()
    for g in dn:
        g.q1()
    hidden(0, 1, 3, 5)
    for g in dn:
        g.q2()
    hidden(1, 2, 0, 1)
    for g in dn:
        g.q3()
    hidden(1, 2, 1, 2)
    for g in dn:
        g.r012()
    for g in dn:
        g.join1()
    down(0, 0)
    push(SB.at[0, pl.ds(0, 8), first], RB.at[0, pl.ds(0, 8)], 8, x_up)
    push(SB.at[0, pl.ds(0, 8), second], RB.at[1, pl.ds(0, 8)], 9, x_down)
    hidden(1, 2, 2, 3)
    for g in dn:
        g.r3()
    for g in dn:
        g.join2()
    down(0, 1)
    push(SB.at[0, pl.ds(8, 8), first], RB.at[0, pl.ds(8, 8)], 14, x_up)
    push(SB.at[0, pl.ds(8, 8), second], RB.at[1, pl.ds(8, 8)], 15, x_down)
    hidden(1, 2, 3, 5)
    down(1, 0)
    push(SB.at[1, pl.ds(0, 8), second], R.at[0, pl.ds(0, 8), second], 10, x_up)
    down(2, 0)
    push(SB.at[2, pl.ds(0, 8), first], R.at[1, pl.ds(0, 8), first], 11, x_down)
    down(1, 1)
    push(SB.at[1, pl.ds(8, 8), second], R.at[0, pl.ds(8, 8), second], 16, x_up)
    down(2, 1)
    push(SB.at[2, pl.ds(8, 8), first], R.at[1, pl.ds(8, 8), first], 17, x_down)
    arrived(RB.at[0, pl.ds(0, 8)], 8)
    relay(1, 0, 0, 0)
    push(SB.at[1, pl.ds(0, 8), first], R.at[0, pl.ds(0, 8), first], 12, x_up)
    arrived(RB.at[1, pl.ds(0, 8)], 9)
    relay(2, 96, 1, 0)
    push(SB.at[2, pl.ds(0, 8), second], R.at[1, pl.ds(0, 8), second], 13, x_down)
    arrived(RB.at[0, pl.ds(8, 8)], 14)
    relay(1, 0, 0, 1)
    push(SB.at[1, pl.ds(8, 8), first], R.at[0, pl.ds(8, 8), first], 18, x_up)
    arrived(RB.at[1, pl.ds(8, 8)], 15)
    relay(2, 96, 1, 1)
    push(SB.at[2, pl.ds(8, 8), second], R.at[1, pl.ds(8, 8), second], 19, x_down)
    hidden(3, 1, 0, 5)
    down(3, 0)
    down(3, 1)

    def last_rows(i, _):
        r = rows16(i)
        total = jnp.zeros((16, LANES), jnp.float32)
        values = []
        for k in range(16):
            v = SB[3, k, r].astype(jnp.float32) + R[0, k, r].astype(jnp.float32) + R[1, k, r].astype(jnp.float32)
            values.append(v)
            total = total + v * v
        scale = lax.rsqrt(jnp.sum(total, axis=-1, keepdims=True) * (1.0 / D) + eps)
        for k in range(16):
            cols = pl.ds(pl.multiple_of((slots[k][0] * 4 + slots[k][1]) * LANES, LANES), LANES)
            a = AM[pl.ds(pl.multiple_of(i * 16 + 16, 16), 16), cols]
            out[r, cols] = (a + values[k] * scale * GAINS[3, :, cols]).astype(jnp.bfloat16)
        return 0

    arrived(R.at[0, pl.ds(0, 8), second], 10)
    arrived(R.at[1, pl.ds(0, 8), first], 11)
    arrived(R.at[0, pl.ds(0, 8), first], 12)
    arrived(R.at[1, pl.ds(0, 8), second], 13)
    arrived(R.at[0, pl.ds(8, 8), second], 16)
    arrived(R.at[1, pl.ds(8, 8), first], 17)
    arrived(R.at[0, pl.ds(8, 8), first], 18)
    arrived(R.at[1, pl.ds(8, 8), second], 19)
    lax.fori_loop(0, ROWS // 16, last_rows, 0, unroll=2)
    with jax.named_scope("drain"):
        pushed(XB.at[pl.ds(0, 3), pl.ds(0, ROWS)], 0)
        pushed(XB.at[0, pl.ds(0, 4 * HALO)], 1)
        pushed(SB.at[pl.ds(0, 3)], 2)
        for both in (pool, gu, dn):
            for g in both:
                g.drain()


def shards(
    tokens,
    mix_gain_in,
    pool_weight,
    mix_gain_out,
    ffn_gain_in,
    gate_weight,
    up_weight,
    gate_taps,
    up_taps,
    down_weight,
    ffn_gain_out,
):
    anywhere = pl.BlockSpec(memory_space=pl.ANY)
    vmem = pl.BlockSpec(memory_space=pltpu.VMEM)
    bf16, f32 = jnp.bfloat16, jnp.float32
    gains = [g.reshape(1, D) for g in (mix_gain_in, mix_gain_out, ffn_gain_in, ffn_gain_out)]
    return pl.pallas_call(
        layer,
        out_shape=jax.ShapeDtypeStruct((ROWS, D), bf16),
        in_specs=[anywhere] * 11,
        out_specs=vmem,
        scratch_shapes=[
            pltpu.VMEM((4, EXT, D), bf16),
            pltpu.VMEM((EXT, LANES), f32),
            pltpu.VMEM((OUTR, D), bf16),
            pltpu.VMEM((OUTR, D), bf16),
            pltpu.VMEM((OUTR, D), f32),
            pltpu.VMEM((4, 4, 4, 32, 512), bf16),
            pltpu.VMEM((4, 4, 128, 2 * GW), bf16),
            pltpu.VMEM((4, 4, GW, LANES), bf16),
            pltpu.VMEM((4, OUTR, D), bf16),
            pltpu.VMEM((2 * OUTR, 256), f32),
            pltpu.VMEM((2 * OUTR, 256), f32),
            pltpu.VMEM((4, ROWS, GW), bf16),
            pltpu.VMEM((4, 16, ROWS, LANES), bf16),
            pltpu.VMEM((2, 16, 96, LANES), bf16),
            pltpu.VMEM((2, 16, ROWS, LANES), bf16),
            pltpu.VMEM((OUTR, D), f32),
            pltpu.VMEM((2, W, LANES), bf16),
            pltpu.VMEM((3, GW), f32),
            pltpu.VMEM((3, GW), f32),
            pltpu.VMEM((8, GW), f32),
            pltpu.VMEM((4, 1, D), f32),
            pltpu.SemaphoreType.DMA((12,)),
            pltpu.SemaphoreType.DMA((6, 5)),
            pltpu.SemaphoreType.DMA((6, 19)),
            pltpu.SemaphoreType.DMA((3,)),
            pltpu.SemaphoreType.DMA((20,)),
        ],
        compiler_params=pltpu.CompilerParams(collective_id=0, has_side_effects=True, vmem_limit_bytes=60 * 1024 * 1024),
    )(tokens, pool_weight, gate_weight.T, up_weight.T, down_weight, gate_taps, up_taps, *gains)


def solution(mesh):
    in_specs = (
        P(("rep", "fs", "tp"), None),
        P(),
        P(None, "fs", None),
        P(),
        P(),
        P("fs", "tp"),
        P("fs", "tp"),
        P(),
        P(),
        P("tp", "fs"),
        P(),
    )
    out_specs = P(("rep", "fs", "tp"), None)
    return jax.shard_map(shards, mesh=mesh, in_specs=in_specs, out_specs=out_specs, check_vma=False)
```

```python
import jax
import jax.numpy as jnp
from jax import lax
from jax.experimental import pallas as pl
from jax.experimental.pallas import tpu as pltpu
from jax.sharding import PartitionSpec as P

MESH = pl.DeviceIdType.MESH
eps = 1e-06
ROWS = 192
HALO = 32
EXT = ROWS + HALO
OUTR = ROWS + 16
D = 2048
W = 704
WP = 768
GW = 2 * W
MAIN = 640
LANES = 128


def ring(value, n):
    return lax.rem(value + n, n)


class Flow:
    def __init__(self, piece, bundle, block, other, p, s, devs, partner, ssem, rsem):
        self.piece, self.bundle, self.block, self.other = piece, bundle, block, other
        self.s = s
        self.columns = [ring(p + k, 4) for k in (0, -1, 1, 2)]
        self.pu, self.pd, self.su, self.sd = devs
        self.partner = partner
        self.ssem, self.rsem = ssem, rsem

    def send(self, ref, dev, k, n):
        pltpu.make_async_remote_copy(
            ref, ref, self.ssem.at[k], self.rsem.at[n], device_id=dev, device_id_type=MESH
        ).start()

    def seen(self, ref, k, n):
        return pltpu.make_async_remote_copy(
            ref, ref, self.ssem.at[k], self.rsem.at[n], device_id=self.partner, device_id_type=MESH
        )

    def recv(self, ref, n):
        self.seen(ref, 0, n).wait_recv()


class Relay(Flow):
    def __init__(self, *args, split):
        super().__init__(*args)
        self.split = split

    def start_p(self):
        own = self.piece(self.columns[0], self.s, None)
        self.send(own, self.pu, 0, 0)
        self.send(own, self.pd, 0, 1)

    def spread(self, j):
        ref = self.piece(self.columns[j], self.s, None)
        self.send(ref, self.su, 2, 3 + 2 * j)
        self.send(ref, self.sd, 2, 4 + 2 * j)

    def start_s(self):
        self.spread(0)

    def give(self, off, k):
        self.send(self.bundle(ring(self.s + off, 4)), self.partner, 4, 12 + k * self.split)

    def p1f(self):
        low, high = self.columns[1], self.columns[2]
        self.recv(self.piece(low, self.s, None), 0)
        self.send(self.piece(low, self.s, 0), self.pu, 1, 2)
        self.recv(self.piece(high, self.s, None), 1)
        self.send(self.piece(high, self.s, 1), self.pd, 1, 2)

    def p1s(self):
        self.spread(1)
        self.spread(2)

    def p2(self):
        self.recv(self.piece(self.columns[3], self.s, None), 2)
        self.spread(3)
        self.give(0, 0)

    def q(self, j):
        col = self.columns[j]
        low, high = ring(self.s - 1, 4), ring(self.s + 1, 4)
        self.recv(self.piece(col, low, None), 3 + 2 * j)
        self.send(self.piece(col, low, 0), self.su, 3, self.landed(j))
        self.recv(self.piece(col, high, None), 4 + 2 * j)
        self.send(self.piece(col, high, 1), self.sd, 3, self.landed(j))
        if j == 3:
            self.give(-1, 1)
            self.give(1, 2)

    def q0(self):
        self.q(0)

    def q1(self):
        self.q(1)

    def q2(self):
        self.q(2)

    def q3(self):
        self.q(3)

    def landed(self, j):
        return 11 if j == 0 else 15 + j

    def far(self, j):
        ref = self.piece(self.columns[j], ring(self.s + 2, 4), None)
        self.recv(ref, self.landed(j))
        self.send(ref, self.partner, 4, 12 + 3 * self.split)

    def r012(self):
        for j in range(3):
            self.far(j)

    def r3(self):
        self.far(3)

    def join(self):
        self.recv(self.other(None), 12)

    def join1(self):
        for k, off in ((0, 0), (1, -1), (2, 1)):
            self.recv(self.other(ring(self.s + off, 4)), 12 + k)

    def join2(self):
        self.recv(self.other(ring(self.s + 2, 4)), 15)

    def drain(self):
        for k, (m, n) in enumerate(((1, 2), (1, 1), (2, 4), (1, 4), (4, 4))):
            self.seen(self.block(m, n), k, 0).wait_send()


def layer(
    tokens, pool_w, gate_w, up_w, dn_w, gate_taps, up_taps, gain0, gain1, gain2, gain3, out,
    XB, SC, GAP, MIX, AF, POOL, GU, DN, X, P0, P1, HID, SB, RB, R, AM, TW, TG, TU, TAPS, GAINS,
    loc_sem, g_ssem, g_rsem, x_ssem, x_rsem,
):
    rep, fs, tp = lax.axis_index("rep"), lax.axis_index("fs"), lax.axis_index("tp")
    zl, y = lax.div(fs, 4), lax.rem(fs, 4)
    z = rep * 4 + zl
    x, c = lax.div(tp, 2), lax.rem(tp, 2)

    def at_y(d):
        return (rep, zl * 4 + ring(y + d, 4), tp)

    def at_z(d):
        zn = ring(z + d, 8)
        return (lax.div(zn, 4), lax.rem(zn, 4) * 4 + y, tp)

    def at_tp(t):
        return (rep, fs, t)

    partner = at_tp(x * 2 + (1 - c))
    x_up, x_down = at_tp(ring(x + 1, 4) * 2 + c), at_tp(ring(x - 1, 4) * 2 + c)
    after = at_tp(ring(tp + 1, 8))
    cross = at_tp(ring(tp + 2 * c - 1, 8))
    y_up, y_down, z_up, z_down = at_y(1), at_y(-1), at_z(1), at_z(-1)

    barrier = pltpu.get_barrier_semaphore()
    greeted = (partner, x_up, x_down, cross, y_up, y_down, z_up, z_down)
    for dev in greeted:
        pl.semaphore_signal(barrier, inc=1, device_id=dev, device_id_type=MESH)

    def cut(start, size, sub):
        start, size = (start, size) if sub is None else (start + sub * (size // 2), size // 2)
        return pl.ds(start if isinstance(start, int) else pl.multiple_of(start, 16), size)

    mine = pl.ds(pl.multiple_of(c * GW, LANES), GW)
    theirs = pl.ds(pl.multiple_of((1 - c) * GW, LANES), GW)
    pairs = [
        (gate_w, TW.at[0]),
        (up_w, TW.at[1]),
        (tokens, XB.at[x, pl.ds(HALO, ROWS)]),
        (pool_w.at[pl.ds(c * 2, 2)], POOL.at[pl.ds(c * 2, 2), zl, y]),
        (dn_w.at[pl.ds(0, MAIN)], DN.at[zl, y, cut(c * WP, MAIN, None)]),
        (dn_w.at[pl.ds(MAIN, 64)], DN.at[zl, y, cut(MAIN + c * 64, 64, None)]),
        (gate_taps.at[:, pl.ds(pl.multiple_of(x * GW, LANES), GW)], TG),
        (up_taps.at[:, pl.ds(pl.multiple_of(x * GW, LANES), GW)], TU),
        (gain0, GAINS.at[0]),
        (gain1, GAINS.at[1]),
        (gain2, GAINS.at[2]),
        (gain3, GAINS.at[3]),
    ]
    local = [pltpu.make_async_copy(src, dst, loc_sem.at[k]) for k, (src, dst) in enumerate(pairs)]
    for copy in local:
        copy.start()
    for k in (2, 3):
        local[k].wait()

    def build():
        for k in (0, 1, 4, 5, 6, 7, 8, 9, 10, 11):
            local[k].wait()
        turned = [TW[k].T for k in range(2)]
        for k in range(2):
            for t in range(5):
                at = pl.multiple_of(c * 1536 + t * 256 + k * LANES, LANES)
                GU[zl, y, :, pl.ds(at, LANES)] = turned[k][:, t * LANES:(t + 1) * LANES]
        ends = [w[:, MAIN:W] for w in turned]
        both = jnp.concatenate([ends[0], ends[1]], axis=1).astype(jnp.float32)
        swapped = jnp.concatenate([ends[1], ends[0]], axis=1).astype(jnp.float32)
        pick = jnp.where(c == 0, both, swapped)
        GU[zl, y, :, pl.ds(pl.multiple_of(1280 + c * LANES, LANES), LANES)] = pick.astype(jnp.bfloat16)
        for ref, base in ((TG, 0), (TU, 3)):
            v = ref[...]
            TAPS[base:base + 3, 0:MAIN] = v[:, 0:MAIN]
            TAPS[base:base + 3, MAIN:WP] = jnp.concatenate([v[:, MAIN:W], v[:, W + MAIN:GW]], axis=1)
            TAPS[base:base + 3, WP:GW] = v[:, W:W + MAIN]

    with jax.named_scope("barrier_wait"):
        pl.semaphore_wait(barrier, len(greeted))

    yz = (y_up, y_down, z_up, z_down)
    zy = (z_up, z_down, y_up, y_down)

    def region(ref, rows, cols=None):
        def at(i, j, sub=None):
            start, size = rows
            here = cut(start, size, sub)
            return ref.at[i, j, here] if cols is None else ref.at[i, j, here, cols]

        return at

    every = slice(None)

    def pair(make, mine_a, mine_b, theirs_a, theirs_b, n, **more):
        def block(at):
            return lambda m, k: at(pl.ds(0, m), pl.ds(0, k))

        return (
            make(
                lambda p, s, sub: mine_a(s, p, sub), lambda s: mine_a(s, every), block(mine_a),
                lambda s: theirs_a(every if s is None else s, every),
                y, zl, yz, partner, g_ssem.at[n], g_rsem.at[n], **more,
            ),
            make(
                lambda p, s, sub: mine_b(p, s, sub), lambda s: mine_b(every, s), block(mine_b),
                lambda s: theirs_b(every, every if s is None else s),
                zl, y, zy, partner, g_ssem.at[n + 1], g_rsem.at[n + 1], **more,
            ),
        )

    pool = pair(
        Relay,
        region(POOL.at[2 * c], (0, 32)), region(POOL.at[2 * c + 1], (0, 32)),
        region(POOL.at[2 * (1 - c)], (0, 32)), region(POOL.at[2 * (1 - c) + 1], (0, 32)),
        0, split=0,
    )
    gu = pair(
        Relay,
        region(GU, (0, 64), mine), region(GU, (64, 64), mine),
        region(GU, (0, 64), theirs), region(GU, (64, 64), theirs),
        2, split=0,
    )
    dn = pair(
        Relay,
        region(DN, (c * W, 352)), region(DN, (c * W + 352, 352)),
        region(DN, ((1 - c) * W, 352)), region(DN, ((1 - c) * W + 352, 352)),
        4, split=1,
    )

    def push(src, dst, k, dev):
        n = 0 if k < 4 else 1 if k < 8 else 2
        pltpu.make_async_remote_copy(
            src, dst, x_ssem.at[n], x_rsem.at[k], device_id=dev, device_id_type=MESH
        ).start()

    def pushed(ref, n):
        pltpu.make_async_remote_copy(
            ref, ref, x_ssem.at[n], x_rsem.at[0], device_id=partner, device_id_type=MESH
        ).wait_send()

    def arrived(dst, k):
        pltpu.make_async_remote_copy(
            dst, dst, x_ssem.at[0], x_rsem.at[k], device_id=partner, device_id_type=MESH
        ).wait_recv()

    low, high, far = ring(x - 1, 4), ring(x + 1, 4), ring(x + 2, 4)
    body = pl.ds(HALO, ROWS)
    head, tail = pl.ds(HALO, 96), pl.ds(HALO + 96, 96)
    last = pl.ds(EXT - HALO, HALO)
    top = pl.ds(0, HALO)

    def side(m, slot):
        push(XB.at[ring(x + 1 - c + m, 4), last], XB.at[slot, top], 5 + m, partner)

    def rows16(i):
        return pl.ds(pl.multiple_of(i * 16, 16), 16)

    def prep(b, first_row):
        at_start = jnp.where(first_row == 0, 0.0, 1.0)
        XB[b, 0:HALO] = (XB[b, 0:HALO].astype(jnp.float32) * at_start).astype(jnp.bfloat16)

        def scales(i, _):
            v = XB[b, rows16(i), :].astype(jnp.float32)
            scale = lax.rsqrt(jnp.mean(v * v, axis=-1, keepdims=True) + eps)
            SC[rows16(i), :] = jnp.broadcast_to(scale, (16, LANES))
            return 0

        lax.fori_loop(0, EXT // 16, scales, 0, unroll=7)
        where = first_row + lax.broadcasted_iota(jnp.int32, (16, LANES), 0)
        for g in range(4):
            span = 2 << g
            inverse = 1.0 / jnp.clip(where + 1, 1, span).astype(jnp.float32)

            def strip(t, _):
                cols = pl.ds(pl.multiple_of(g * 512 + t * LANES, LANES), LANES)
                v = XB[b, :, cols].astype(jnp.float32) * SC[...] * GAINS[0, :, cols]
                v = v.astype(jnp.bfloat16).astype(jnp.float32)
                total = v
                for k in range(g + 1):
                    total = total + pltpu.roll(total, 1 << k, 0)
                GAP[0:16, cols] = (total[16:32] * (1.0 / span) - v[16:32]).astype(jnp.bfloat16)
                GAP[16:32, cols] = (total[32:48] * inverse - v[32:48]).astype(jnp.bfloat16)
                GAP[32:OUTR, cols] = (total[48:] * (1.0 / span) - v[48:]).astype(jnp.bfloat16)
                return 0

            lax.fori_loop(0, 4, strip, 0)

    def post(b, n, keep):
        for g in range(4):
            cols = slice(g * 512, (g + 1) * 512)
            MIX[:, cols] = jnp.dot(
                GAP[:, cols], POOL[g].reshape(512, 512), preferred_element_type=jnp.float32
            ).astype(jnp.bfloat16)

        def scales(i, _):
            v = MIX[rows16(i), :].astype(jnp.float32)
            scale = lax.rsqrt(jnp.mean(v * v, axis=-1, keepdims=True) + eps)
            SC[rows16(i), :] = jnp.broadcast_to(scale, (16, LANES))
            return 0

        lax.fori_loop(0, OUTR // 16, scales, 0, unroll=13)

        def added(i, _):
            total = jnp.zeros((16, LANES), jnp.float32)
            scale = SC[rows16(i), :]
            for t in range(D // LANES):
                cols = slice(t * LANES, (t + 1) * LANES)
                v = MIX[rows16(i), cols].astype(jnp.float32)
                rows = pl.ds(pl.multiple_of(i * 16 + 16, 16), 16)
                a = XB[b, rows, cols].astype(jnp.float32) + v * scale * GAINS[1, :, cols]
                keep[rows16(i), cols] = a
                total = total + a * a
            scale = lax.rsqrt(jnp.sum(total, axis=-1, keepdims=True) * (1.0 / D) + eps)
            SC[rows16(i), :] = jnp.broadcast_to(scale, (16, LANES))
            return 0

        lax.fori_loop(0, OUTR // 16, added, 0)

        def scaled(i, _):
            scale = SC[rows16(i), :]
            for t in range(D // LANES):
                cols = slice(t * LANES, (t + 1) * LANES)
                X[n, rows16(i), cols] = (keep[rows16(i), cols] * scale * GAINS[2, :, cols]).astype(jnp.bfloat16)
            return 0

        lax.fori_loop(0, OUTR // 16, scaled, 0)

    def start_of(b):
        return (2 * b + c) * ROWS

    def hidden(n, count, begin, stop):
        size = count * OUTR
        left = X[n] if count == 1 else X[n:n + count].reshape(size, D)

        def project(i, ref):
            w = GU[:, :, :, pl.ds(pl.multiple_of(i * 256, 256), 256)].reshape(D, 256)
            pre = jnp.dot(left, w, preferred_element_type=jnp.float32).astype(jnp.bfloat16).astype(jnp.float32)
            ref[0:size, :] = pre

        def conv(v, taps_at, base):
            taps = TAPS[base:base + 3, pl.ds(taps_at, LANES)]
            return taps[0:1] * pltpu.roll(v, 2, 0) + taps[1:2] * pltpu.roll(v, 1, 0) + taps[2:3] * v

        def act(ref, i, ends):
            at = i * LANES if ends else pl.multiple_of(i * LANES, LANES)
            for k in range(count):
                for row in (0, 96):
                    here = slice(k * OUTR + row, k * OUTR + row + 112)
                    gate, up = ref[here, 0:LANES], ref[here, LANES:]
                    if ends:
                        lead = lax.broadcasted_iota(jnp.int32, (112, LANES), 1) < 64
                        gate, up = jnp.where(lead, gate, up), pltpu.roll(jnp.where(lead, up, gate), 64, 1)
                    gate, up = conv(gate, at, 0)[16:], conv(up, at, 3)[16:]
                    inner = 0.7978845608028654 * (gate + 0.044715 * gate * gate * gate)
                    value = 0.5 * gate * (1.0 + jnp.tanh(inner)) * up
                    HID[n + k, row:row + 96, pl.ds(at, LANES)] = value.astype(jnp.bfloat16)

        def order(i):
            return i + jnp.minimum(lax.div(i, 5), 1) - 6 * lax.div(i, 10)

        if begin == 0:
            project(0, P0)

        def two(i, _):
            project(order(2 * i + 1), P1)
            act(P0, order(2 * i), False)
            project(order(2 * i + 2), P0)
            act(P1, order(2 * i + 1), False)
            return 0

        lax.fori_loop(begin, stop, two, 0)
        if stop == 5:
            act(P0, 5, True)

    steps = [(0, 0), (0, 1), (0, -1), (1, 0), (-1, 0), (1, 1), (1, -1), (-1, 1)]
    steps += [(-1, -1), (2, 0), (2, 1), (2, -1), (0, 2), (1, 2), (-1, 2), (2, 2)]
    slots = [(ring(zl + dz, 4), ring(y + dy, 4)) for dz, dy in steps]

    def down(b, part):
        for k in range(8 * part, 8 * part + 8, 2):
            w = jnp.concatenate([DN[slots[k]], DN[slots[k + 1]]], axis=1)
            total = jnp.dot(HID[b], w, preferred_element_type=jnp.float32).astype(jnp.bfloat16)
            SB[b, k] = total[:, 0:LANES]
            SB[b, k + 1] = total[:, LANES:]

    def relay(b, start, k, part):
        rows = pl.ds(start, 96)

        def add(i, _):
            SB[b, i, rows] = (SB[b, i, rows].astype(jnp.float32) + RB[k, i].astype(jnp.float32)).astype(jnp.bfloat16)
            return 0

        lax.fori_loop(8 * part, 8 * part + 8, add, 0)

    first, second = pl.ds(0, 96), pl.ds(96, 96)
    push(XB.at[x, last], XB.at[ring(x + c, 4), top], 4, after)
    for g in pool:
        g.start_p()
    for g in pool:
        g.start_s()
    push(XB.at[x, body], XB.at[x, body], 0, x_up)
    push(XB.at[x, body], XB.at[x, body], 1, x_down)
    build()
    for g in gu:
        g.start_p()
    for g in pool:
        g.p1f()
    for g in pool:
        g.p1s()
    arrived(XB.at[x, top], 4)
    prep(x, start_of(x))
    for g in pool:
        g.p2()
    for g in pool:
        g.q0()
    for g in pool:
        g.q1()
    for g in pool:
        g.q2()
    for g in gu:
        g.start_s()
    for g in gu:
        g.p1f()
    for g in pool:
        g.q3()
    for g in gu:
        g.p1s()
    for g in pool:
        g.r012()
    for g in pool:
        g.r3()
    arrived(XB.at[low, body], 0)
    push(XB.at[low, head], XB.at[low, head], 2, x_up)
    arrived(XB.at[high, body], 1)
    push(XB.at[high, tail], XB.at[high, tail], 3, x_down)
    side(0, high)
    for g in pool:
        g.join()
    post(x, 3, AM)
    for g in gu:
        g.p2()
    for g in gu:
        g.q0()
    arrived(XB.at[high, top], 5)
    prep(high, start_of(high))
    post(high, 1, AF)
    for g in gu:
        g.q1()
    for g in dn:
        g.start_p()
    for g in gu:
        g.q2()
    arrived(XB.at[far, head], 2)
    arrived(XB.at[far, tail], 3)
    side(1, far)
    side(2, low)
    arrived(XB.at[far, top], 6)
    for g in gu:
        g.q3()
    for g in dn:
        g.start_s()
    prep(far, start_of(far))
    post(far, 0, AF)
    arrived(XB.at[low, top], 7)
    prep(low, start_of(low))
    for g in dn:
        g.p1f()
    for g in dn:
        g.p1s()
    post(low, 2, AF)
    for g in gu:
        g.r012()
    for g in gu:
        g.r3()
    for g in gu:
        g.join()
    hidden(0, 1, 0, 1)
    for g in dn:
        g.p2()
    hidden(0, 1, 1, 3)
    for g in dn:
        g.q0()
    for g in dn:
        g.q1()
    hidden(0, 1, 3, 5)
    for g in dn:
        g.q2()
    hidden(1, 2, 0, 1)
    for g in dn:
        g.q3()
    hidden(1, 2, 1, 2)
    for g in dn:
        g.r012()
    for g in dn:
        g.join1()
    down(0, 0)
    push(SB.at[0, pl.ds(0, 8), first], RB.at[0, pl.ds(0, 8)], 8, x_up)
    push(SB.at[0, pl.ds(0, 8), second], RB.at[1, pl.ds(0, 8)], 9, x_down)
    hidden(1, 2, 2, 3)
    for g in dn:
        g.r3()
    for g in dn:
        g.join2()
    down(0, 1)
    push(SB.at[0, pl.ds(8, 8), first], RB.at[0, pl.ds(8, 8)], 14, x_up)
    push(SB.at[0, pl.ds(8, 8), second], RB.at[1, pl.ds(8, 8)], 15, x_down)
    hidden(1, 2, 3, 5)
    down(1, 0)
    push(SB.at[1, pl.ds(0, 8), second], R.at[0, pl.ds(0, 8), second], 10, x_up)
    down(2, 0)
    push(SB.at[2, pl.ds(0, 8), first], R.at[1, pl.ds(0, 8), first], 11, x_down)
    down(1, 1)
    push(SB.at[1, pl.ds(8, 8), second], R.at[0, pl.ds(8, 8), second], 16, x_up)
    down(2, 1)
    push(SB.at[2, pl.ds(8, 8), first], R.at[1, pl.ds(8, 8), first], 17, x_down)
    arrived(RB.at[0, pl.ds(0, 8)], 8)
    relay(1, 0, 0, 0)
    push(SB.at[1, pl.ds(0, 8), first], R.at[0, pl.ds(0, 8), first], 12, x_up)
    arrived(RB.at[1, pl.ds(0, 8)], 9)
    relay(2, 96, 1, 0)
    push(SB.at[2, pl.ds(0, 8), second], R.at[1, pl.ds(0, 8), second], 13, x_down)
    arrived(RB.at[0, pl.ds(8, 8)], 14)
    relay(1, 0, 0, 1)
    push(SB.at[1, pl.ds(8, 8), first], R.at[0, pl.ds(8, 8), first], 18, x_up)
    arrived(RB.at[1, pl.ds(8, 8)], 15)
    relay(2, 96, 1, 1)
    push(SB.at[2, pl.ds(8, 8), second], R.at[1, pl.ds(8, 8), second], 19, x_down)
    hidden(3, 1, 0, 5)
    down(3, 0)
    down(3, 1)

    def summed(k, r):
        return SB[3, k, r].astype(jnp.float32) + R[0, k, r].astype(jnp.float32) + R[1, k, r].astype(jnp.float32)

    def first_rows(i, _):
        r = rows16(i)
        total = jnp.zeros((16, LANES), jnp.float32)
        for k in range(8):
            v = summed(k, r)
            AF[r, k * LANES:(k + 1) * LANES] = v
            total = total + v * v
        SC[r, :] = total
        return 0

    def last_rows(i, _):
        r = rows16(i)
        total = SC[r, :]
        values = []
        for k in range(8, 16):
            v = summed(k, r)
            values.append(v)
            total = total + v * v
        scale = lax.rsqrt(jnp.sum(total, axis=-1, keepdims=True) * (1.0 / D) + eps)
        for k in range(16):
            cols = pl.ds(pl.multiple_of((slots[k][0] * 4 + slots[k][1]) * LANES, LANES), LANES)
            a = AM[pl.ds(pl.multiple_of(i * 16 + 16, 16), 16), cols]
            v = AF[r, k * LANES:(k + 1) * LANES] if k < 8 else values[k - 8]
            out[r, cols] = (a + v * scale * GAINS[3, :, cols]).astype(jnp.bfloat16)
        return 0

    for p in range(2):
        here = pl.ds(8 * p, 8)
        arrived(R.at[0, here, second], 10 + 6 * p)
        arrived(R.at[1, here, first], 11 + 6 * p)
        arrived(R.at[0, here, first], 12 + 6 * p)
        arrived(R.at[1, here, second], 13 + 6 * p)
        lax.fori_loop(0, ROWS // 16, last_rows if p else first_rows, 0, unroll=2)
    with jax.named_scope("drain"):
        pushed(XB.at[pl.ds(0, 3), pl.ds(0, ROWS)], 0)
        pushed(XB.at[0, pl.ds(0, 4 * HALO)], 1)
        pushed(SB.at[pl.ds(0, 3)], 2)
        for both in (pool, gu, dn):
            for g in both:
                g.drain()


def shards(
    tokens,
    mix_gain_in,
    pool_weight,
    mix_gain_out,
    ffn_gain_in,
    gate_weight,
    up_weight,
    gate_taps,
    up_taps,
    down_weight,
    ffn_gain_out,
):
    anywhere = pl.BlockSpec(memory_space=pl.ANY)
    vmem = pl.BlockSpec(memory_space=pltpu.VMEM)
    bf16, f32 = jnp.bfloat16, jnp.float32
    gains = [g.reshape(1, D) for g in (mix_gain_in, mix_gain_out, ffn_gain_in, ffn_gain_out)]
    return pl.pallas_call(
        layer,
        out_shape=jax.ShapeDtypeStruct((ROWS, D), bf16),
        in_specs=[anywhere] * 11,
        out_specs=vmem,
        scratch_shapes=[
            pltpu.VMEM((4, EXT, D), bf16),
            pltpu.VMEM((EXT, LANES), f32),
            pltpu.VMEM((OUTR, D), bf16),
            pltpu.VMEM((OUTR, D), bf16),
            pltpu.VMEM((OUTR, D), f32),
            pltpu.VMEM((4, 4, 4, 32, 512), bf16),
            pltpu.VMEM((4, 4, 128, 2 * GW), bf16),
            pltpu.VMEM((4, 4, GW, LANES), bf16),
            pltpu.VMEM((4, OUTR, D), bf16),
            pltpu.VMEM((2 * OUTR, 256), f32),
            pltpu.VMEM((2 * OUTR, 256), f32),
            pltpu.VMEM((4, ROWS, GW), bf16),
            pltpu.VMEM((4, 16, ROWS, LANES), bf16),
            pltpu.VMEM((2, 16, 96, LANES), bf16),
            pltpu.VMEM((2, 16, ROWS, LANES), bf16),
            pltpu.VMEM((OUTR, D), f32),
            pltpu.VMEM((2, W, LANES), bf16),
            pltpu.VMEM((3, GW), f32),
            pltpu.VMEM((3, GW), f32),
            pltpu.VMEM((8, GW), f32),
            pltpu.VMEM((4, 1, D), f32),
            pltpu.SemaphoreType.DMA((12,)),
            pltpu.SemaphoreType.DMA((6, 5)),
            pltpu.SemaphoreType.DMA((6, 19)),
            pltpu.SemaphoreType.DMA((3,)),
            pltpu.SemaphoreType.DMA((20,)),
        ],
        compiler_params=pltpu.CompilerParams(collective_id=0, has_side_effects=True, vmem_limit_bytes=60 * 1024 * 1024),
    )(tokens, pool_weight, gate_weight.T, up_weight.T, down_weight, gate_taps, up_taps, *gains)


def solution(mesh):
    in_specs = (
        P(("rep", "fs", "tp"), None),
        P(),
        P(None, "fs", None),
        P(),
        P(),
        P("fs", "tp"),
        P("fs", "tp"),
        P(),
        P(),
        P("tp", "fs"),
        P(),
    )
    out_specs = P(("rep", "fs", "tp"), None)
    return jax.shard_map(shards, mesh=mesh, in_specs=in_specs, out_specs=out_specs, check_vma=False)
```
